256 devices in a mesh: grp: 2 (over y), sp: 16 (over z), tp: 8 (over x, core).
Axes of the slice: x: 4, y: 2, z: 16, core: 2. Of those that a mesh axis runs over, the one named last changes fastest.
The devices are a block of a 4x16x16 slice.
Arguments:
- tokens: bfloat16 [65536, 2048], P(('grp', 'sp')), parts along dimension 0, may hold values from -6 to 6
- in_gain: float32 [2048], replicated, may hold values from 0.1 to 1.9
- w_input: bfloat16 [2048, 2048], P(None, 'tp'), may hold values from -0.125 to 0.125
- w_gate: bfloat16 [2048, 2048], P(None, 'tp'), may hold values from -4 to 4
- conv_taps: float32 [4, 2048], P(None, 'tp'), may hold values from -3 to 3
- w_rate: bfloat16 [8, 256, 256], P('tp'), may hold values from -0.375 to 0.375
- w_inlet: bfloat16 [8, 256, 256], P('tp'), may hold values from -0.375 to 0.375
- decay_param: float32 [2048], P('tp'), may hold values from 3 to 25
- decay_bias: float32 [8, 65536], P('tp', ('grp', 'sp')), parts along dimension 1, may hold values from -1.5 to 0
- out_gain: float32 [2048], P('tp'), may hold values from 0.1 to 1.9
- w_out: bfloat16 [2048, 2048], P('sp'), may hold values from -0.125 to 0.125
Outputs:
- mixer_out: bfloat16 [65536, 2048], P(('grp', 'sp', 'tp')), parts along dimension 0
The draws below stay inside these ranges and needn't reach their ends.
There are 2 independent parts, one for each index of `grp`. The reference program is written for one: setup_inputs(seed, part) draws one part's arguments, and reference() takes and returns one part's arrays. A program takes and returns all parts, laid end to end along the dimension named above; an argument that names none is the same for every part. Nothing has to cross between parts.
All inputs are finite; a program needn't handle non-finite values.
Results may differ from the reference program's by a relative error of at most 0.013.
Values may be sent and summed in bfloat16 or wider, within the bound.
No kernel may reach another device: no remote copies, remote signals or barrier semaphores. Data moves between devices by JAX's collectives and lax.ppermute only.
A program may use at most 128 MiB of HBM per device.

```python
import math
import jax
import jax.numpy as jnp
from jax import lax

D = 2048
HEADS = 8
HEAD = 256
CONV = 4
SEQ_DEV = 2048
DR = 2048
SEQ = 32768


def draw_w_gate(key, part):
    base_key, jitter_key = jax.random.split(jax.random.fold_in(key, 11))
    columns = HEADS * HEAD
    base = jnp.clip(jax.random.normal(base_key, (D, columns), jnp.float32), -4.0, 4.0)
    position = jnp.arange(columns, dtype=jnp.float32) / columns
    jitter = jax.random.uniform(jitter_key, (columns,), jnp.float32) / HEADS
    column_scale = jnp.exp((position + jitter) * math.log(6.0))
    return (base * column_scale[None, :] / math.sqrt(D)).astype(jnp.bfloat16)


def draw_decay_param(key, part):
    pick_key, slow_key, fast_key = jax.random.split(jax.random.fold_in(key, 23), 3)
    channels = HEADS * HEAD
    slow = jax.random.bernoulli(pick_key, 0.5, (channels,))
    slow_rate = jax.random.uniform(slow_key, (channels,), jnp.float32, 0.2, 0.6) / (8.0 * SEQ)
    fast_rate = jnp.exp(jax.random.uniform(fast_key, (channels,), jnp.float32, math.log(1.0 / 400.0), math.log(1.0 / 120.0)))
    chosen = jnp.where(slow, slow_rate, fast_rate)
    return -jnp.log(jnp.expm1(chosen))


def draw_decay_bias(key, part):
    span_key, spot_key, depth_key = jax.random.split(jax.random.fold_in(key, 37), 3)
    span_count = SEQ // SEQ_DEV
    level = jnp.exp(jax.random.uniform(span_key, (HEADS, span_count), jnp.float32, math.log(0.2), math.log(1.2))) / SEQ
    dispersion = jnp.repeat(-level, SEQ_DEV, axis=1)
    spots = jax.random.randint(spot_key, (HEADS, 2), 0, SEQ)
    layer_count = jnp.log(jax.random.uniform(depth_key, (HEADS, 2), jnp.float32, 0.55, 0.8))
    match_count = (jnp.arange(SEQ, dtype=jnp.int32)[None, None, :] == spots[:, :, None]).astype(jnp.float32)
    pulse_train = jnp.sum(match_count * layer_count[:, :, None], axis=1)
    return dispersion + pulse_train


def level_of(key, dims, shards, least, top_value):
    factor_of = 1.0
    for dim, parts in shards:
        heights = jax.random.uniform(jax.random.fold_in(jax.random.fold_in(key, 6), dim), (parts,), jnp.float32, least / len(shards), top_value / len(shards))
        factor_of = factor_of * jnp.repeat(jnp.exp(heights), dims[dim] // parts).reshape((-1,) + (1,) * (len(dims) - 1 - dim))
    return factor_of


def scatter_about(key, dims, deviation, reach, shards=(), held_as=jnp.bfloat16):
    factor_of = level_of(key, dims, shards, -0.22, 0.18) if shards else 1.0
    drawn = jax.random.normal(key, dims, jnp.float32) * deviation * factor_of
    return jnp.minimum(jnp.maximum(drawn, -reach), reach).astype(held_as)


def setup_inputs(seed: int = 0, part: int = 0) -> dict:
    key_of = jax.random.split(jax.random.key(seed), 12)
    own_keys = jax.random.split(jax.random.fold_in(key_of[11], part), 12)
    return {
        "tokens": scatter_about(own_keys[0], (SEQ, D), 1.0, 6.0, ((0, 16),)),
        "in_gain": jnp.clip(1.0 + 0.18 * jax.random.normal(key_of[1], (D,), jnp.float32), 0.1, 1.9),
        "w_input": scatter_about(key_of[2], (D, DR), D ** -0.5, 0.125, ((1, 8),)),
        "w_gate": draw_w_gate(jax.random.fold_in(key_of[11], 71), part),
        "conv_taps": scatter_about(key_of[4], (CONV, DR), 0.5, 3.0, ((1, 8),), jnp.float32),
        "w_rate": scatter_about(key_of[5], (HEADS, HEAD, HEAD), HEAD ** -0.5, 0.375, ((0, 8),)),
        "w_inlet": scatter_about(key_of[6], (HEADS, HEAD, HEAD), HEAD ** -0.5, 0.375, ((0, 8),)),
        "decay_param": draw_decay_param(jax.random.fold_in(key_of[11], 71), part),
        "decay_bias": draw_decay_bias(jax.random.fold_in(jax.random.fold_in(key_of[11], part), 71), part),
        "out_gain": jnp.clip(1.0 + 0.18 * jax.random.normal(key_of[9], (DR,), jnp.float32), 0.1, 1.9),
        "w_out": scatter_about(key_of[10], (DR, D), DR ** -0.5, 0.125, ((0, 16),)),
    }


def combine_pairs(first_pair, second_pair):
    return (first_pair[0] * second_pair[0], second_pair[0] * first_pair[1] + second_pair[1])

def reference(tokens, in_gain, w_input, w_gate, conv_taps, w_rate, w_inlet, decay_param, decay_bias, out_gain, w_out):
    seq_len = tokens.shape[0]
    as_float = tokens.astype(jnp.float32)
    inv_norm = lax.rsqrt(lax.optimization_barrier(jnp.mean(as_float * as_float, axis=1, keepdims=True)) + 1e-06)
    normed = (as_float * inv_norm * in_gain).astype(jnp.bfloat16)
    projected = jnp.dot(normed, w_input, preferred_element_type=jnp.float32).astype(jnp.bfloat16)
    gate_raw = jnp.dot(normed, w_gate, preferred_element_type=jnp.float32).astype(jnp.bfloat16)
    padded = jnp.pad(projected.astype(jnp.float32), ((CONV - 1, 0), (0, 0)))
    tap_values = conv_taps.astype(jnp.float32)
    summed = padded[0:seq_len] * tap_values[0]
    for offset in range(1, CONV):
        summed = summed + padded[offset:offset + seq_len] * tap_values[offset]
    convolved = summed.astype(jnp.bfloat16)
    per_head = convolved.astype(jnp.float32).reshape(seq_len, HEADS, HEAD)
    rate_gate = jax.nn.sigmoid(jnp.einsum('shi,hij->shj', per_head, w_rate.astype(jnp.float32))).reshape(seq_len, HEADS * HEAD)
    input_gate = jax.nn.sigmoid(jnp.einsum('shi,hij->shj', per_head, w_inlet.astype(jnp.float32))).reshape(seq_len, HEADS * HEAD)
    head_bias = jnp.repeat(jnp.transpose(decay_bias), HEAD, axis=1)
    log_decay = -8.0 * rate_gate * jax.nn.softplus(-decay_param) + head_bias
    drive_term = jnp.sqrt(-jnp.expm1(2.0 * log_decay)) * input_gate * convolved.astype(jnp.float32)
    decay_prod, full_state = lax.associative_scan(combine_pairs, (jnp.exp(log_decay), drive_term), axis=0)
    gated_out = full_state * jax.nn.gelu(gate_raw.astype(jnp.float32))
    out_scale = lax.rsqrt(lax.optimization_barrier(jnp.mean(gated_out * gated_out, axis=1, keepdims=True)) + 1e-06)
    normed_out = (gated_out * out_scale * out_gain).astype(jnp.bfloat16)
    return jnp.dot(normed_out, w_out, preferred_element_type=jnp.float32).astype(jnp.bfloat16)
```

```python
import functools

import jax
import jax.numpy as jnp
from jax import lax
from jax.experimental import pallas as pl
from jax.experimental.pallas import tpu as pltpu
from jax.sharding import PartitionSpec as P

F32 = jnp.float32
BF16 = jnp.bfloat16
BLOCK = 256
SEG = 8
EXTRA = 16
EPS = 1e-06


def normed_rows(rows, gain):
    wide = rows.astype(F32)
    inv = lax.rsqrt(jnp.mean(wide * wide, axis=1, keepdims=True) + EPS)
    return (wide * inv * gain).astype(BF16)


def minus_expm1(y, exp_y):
    series = 1.0 / 120.0 + y * (1.0 / 720.0)
    series = 1.0 / 24.0 + y * series
    series = 1.0 / 6.0 + y * series
    series = 0.5 + y * series
    series = -y * (1.0 + y * series)
    return jnp.where(y > -0.25, series, 1.0 - exp_y)


def gelu(x):
    inner = 0.7978845608028654 * (x + 0.044715 * (x * x * x))
    return 0.5 * x * (1.0 + jnp.tanh(inner))


def logistic(x):
    return 1.0 / (1.0 + jnp.exp(-x))


def shifted_down(x, by, fill):
    rows = lax.broadcasted_iota(jnp.int32, x.shape, 0)
    return jnp.where(rows < by, fill, pltpu.roll(x, by, 0))


def input_kernel(tokens, gain, w_input, projected):
    normed = normed_rows(tokens[...], gain[...])
    projected[...] = jnp.dot(normed, w_input[...], preferred_element_type=F32).astype(BF16)


def gate_kernel(tokens, gain, w_gate, gate):
    normed = normed_rows(tokens[...], gain[...])
    gate_raw = jnp.dot(normed, w_gate[...], preferred_element_type=F32).astype(BF16)
    gate[...] = gelu(gate_raw.astype(F32))


def thirds(x):
    top = x.astype(BF16)
    rest = x - top.astype(F32)
    middle = rest.astype(BF16)
    return [top, middle, (rest - middle.astype(F32)).astype(BF16)]


def recur_kernel(projected, taps, w_rate, w_inlet, soft, bias, *refs, first):
    early, refs = refs[:3] if first else refs[:4], refs[3:] if first else refs[4:]
    state, prod, ends, conv_buf, decay_buf, drive_buf, carry = refs
    step = pl.program_id(0)

    @pl.when(step == 0)
    def _():
        if first:
            halo, gain, w_input = early
            edge = jnp.dot(normed_rows(halo[...], gain[...]), w_input[...], preferred_element_type=F32)
            conv_buf[0:8, :] = edge.astype(BF16).astype(F32)[8:16]
            head_row = lax.broadcasted_iota(jnp.int32, carry.shape, 0) == 0
            carry[...] = jnp.where(head_row, 1.0, 0.0)
        else:
            before, begun = early[0], early[1]
            conv_buf[0:8, :] = before[...].astype(F32)[8:16]
            carry[...] = begun[0]

    @pl.when(step > 0)
    def _():
        conv_buf[0:8, :] = conv_buf[BLOCK : BLOCK + 8, :]

    conv_buf[8 : BLOCK + 8, :] = projected[...].astype(F32)
    summed = conv_buf[5 : BLOCK + 5, :] * taps[0:1, :]
    for k in range(1, 4):
        summed = summed + conv_buf[5 + k : BLOCK + 5 + k, :] * taps[k : k + 1, :]
    convolved = summed.astype(BF16)
    rate = logistic(jnp.dot(convolved, w_rate[0], preferred_element_type=F32))
    inlet = logistic(jnp.dot(convolved, w_inlet[0], preferred_element_type=F32))
    row_bias = bias[...]
    pieces = thirds(row_bias) + [jnp.zeros((13, BLOCK), BF16)]
    bias_col = lax.dot_general(
        jnp.concatenate(pieces, 0), jnp.ones((16, rate.shape[1]), BF16), (((0,), (0,)), ((), ())),
        preferred_element_type=F32,
    )
    log_decay = -8.0 * rate * soft[...] + bias_col
    decay = jnp.exp(log_decay)
    drive = jnp.sqrt(minus_expm1(2.0 * log_decay, decay * decay)) * inlet * convolved.astype(F32)
    segs = BLOCK // SEG
    for half in range(2):
        lanes = slice(half * 128, half * 128 + 128)
        decay_buf[half] = decay[:, lanes]
        drive_buf[half] = drive[:, lanes]
        row = [(half, pl.ds(r, segs, stride=SEG), slice(None)) for r in range(SEG)]
        p, h = decay_buf[row[0]], drive_buf[row[0]]
        inner = [(p, h)]
        for r in range(1, SEG):
            a = decay_buf[row[r]]
            h = a * h + drive_buf[row[r]]
            p = a * p
            inner.append((p, h))
        by = 1
        while by < segs:
            h = h + p * shifted_down(h, by, 0.0)
            p = p * shifted_down(p, by, 1.0)
            by *= 2
        before_p = shifted_down(p, 1, 1.0)
        before_h = shifted_down(h, 1, 0.0)
        start_h = before_h + before_p * carry[1:2, lanes]
        start_p = before_p * carry[0:1, lanes]
        for r in range(SEG):
            p, h = inner[r]
            state[row[r]] = h + p * start_h
            prod[row[r]] = p * start_p
        carry[0:1, lanes] = prod[half, BLOCK - 1 : BLOCK, :]
        carry[1:2, lanes] = state[half, BLOCK - 1 : BLOCK, :]
    ends[...] = jnp.broadcast_to(carry[...][None], ends.shape)


def gated_kernel(state, prod, gate, ends, gain, sent, incoming):
    @pl.when(pl.program_id(0) == 0)
    def _():
        span = lax.axis_index("sp")
        total = jnp.zeros((1, gain.shape[1]), F32)
        for k in range(ends.shape[0]):
            total = jnp.where(k < span, ends[k, 0:1, :] * total + ends[k, 1:2, :], total)
        incoming[...] = jnp.broadcast_to(total, incoming.shape)

    ones = jnp.ones((8, 128), BF16)
    over = (((1,), (1,)), ((), ()))
    for d in range(sent.shape[0]):
        rows = slice(d * BLOCK, d * BLOCK + BLOCK)
        total = jnp.zeros((8, BLOCK), F32)
        for half in range(2):
            lanes = slice(half * 128, half * 128 + 128)
            gated = (state[half, rows, :] + prod[half, rows, :] * incoming[0:1, lanes]) * gate[rows, lanes]
            sent[d, half, 0:BLOCK, :] = (gated * gain[:, lanes]).astype(BF16)
            square = gated * gated
            high = square.astype(BF16)
            low = (square - high.astype(F32)).astype(BF16)
            total = total + lax.dot_general(ones, high, over, preferred_element_type=F32)
            total = total + lax.dot_general(ones, low, over, preferred_element_type=F32)
        top = total.astype(BF16).astype(F32)
        row = lax.broadcasted_iota(jnp.int32, total.shape, 0)
        lines = jnp.where(row == 0, top, jnp.where(row == 1, total - top, 0.0))
        lines = jnp.concatenate([lines, jnp.zeros_like(lines)], 0).astype(BF16)
        for half in range(2):
            sent[d, half, BLOCK : BLOCK + EXTRA, :] = lines[:, half * 128 : half * 128 + 128]


def product(arrived, places, blocks, low, step):
    mixed = jnp.concatenate([arrived[place, 0:BLOCK, :] for place in places], 1)
    weights = jnp.concatenate([block[:, low : low + step] for block in blocks], 0)
    return jnp.dot(mixed, weights, preferred_element_type=F32)


def places_of(offsets, spans):
    span, core = lax.axis_index("sp"), lax.axis_index("tp") % 2
    return [lax.rem(span + spans + jnp.where(core == 0, k, -k), spans) for k in offsets]


def early_kernel(arrived, *refs, offsets, spans):
    blocks, out = refs[:-1], refs[-1]
    places = places_of(offsets, spans)
    step = 512
    for low in range(0, out.shape[1], step):
        out[:, low : low + step] = product(arrived, places, blocks, low, step)


def late_kernel(arrived, sums, *refs, offsets, spans, channels):
    blocks, out = refs[:-1], refs[-1]
    places = places_of(offsets, spans)
    ones = jnp.ones((arrived.shape[0] // 2 * EXTRA, 128), BF16)
    square = []
    for half in range(2):
        lines = [arrived[k, BLOCK : BLOCK + EXTRA, :] for k in range(half, arrived.shape[0], 2)]
        square.append(
            lax.dot_general(
                jnp.concatenate(lines, 0), ones, (((0,), (0,)), ((), ())), preferred_element_type=F32
            )
        )
    scale = lax.rsqrt(jnp.concatenate(square, 0)[:, 0:1] / channels + EPS)
    step = 512
    for low in range(0, out.shape[1], step):
        acc = sums[:, low : low + step] + product(arrived, places, blocks, low, step)
        out[:, low : low + step] = (acc * scale).astype(BF16)


def tie(*values):
    return lax.optimization_barrier(values)


def body(
    tokens, in_gain, w_input, w_gate, conv_taps, w_rate, w_inlet, decay_param, decay_bias, out_gain, w_out
):
    rows, width = tokens.shape
    head = w_input.shape[1]
    spans, heads = lax.axis_size("sp"), lax.axis_size("tp")
    _, out_width = w_out.shape
    reach = spans // 2

    around = []
    swap = []
    for z in range(spans):
        for t in range(heads):
            ahead = (z + 1) % spans if t % 2 == 0 else (z - 1) % spans
            around.append((z * heads + t, ahead * heads + t))
            swap.append((z * heads + t, z * heads + t + 1 - 2 * (t % 2)))

    moved, swapped = [], []

    def onward(x):
        moved.append(lax.ppermute(x, ("sp", "tp"), around))

    def across(x):
        swapped.append(lax.ppermute(x, ("sp", "tp"), swap))

    def advance(value):
        if swapped:
            value, moved[-1], swapped[-1] = tie(value, moved[-1], swapped[-1])
        else:
            value, moved[-1] = tie(value, moved[-1])
        if len(moved) < reach:
            across(moved[-1])
            onward(moved[-1])
        return value

    fixed = lambda *shape: pl.BlockSpec(shape, lambda i: (0,) * len(shape))
    halves = lambda n, at: pl.BlockSpec((2, n, head // 2), lambda i: (0, i + at, 0))
    moving = lambda n, cols, at=0: pl.BlockSpec((n, cols), lambda i: (i + at, 0))
    hbm = pl.BlockSpec(memory_space=pl.ANY)
    vmem = pl.BlockSpec(memory_space=pltpu.VMEM)

    onward(w_out)
    halo = lax.ppermute(tokens[rows - 16 :], "sp", [(i, i + 1) for i in range(spans - 1)])
    soft = jax.nn.softplus(-decay_param).reshape(1, head)
    gain_row = in_gain.reshape(1, width)

    big = 2 * BLOCK
    projected = pl.pallas_call(
        input_kernel,
        grid=(rows // big,),
        in_specs=[moving(big, width), fixed(1, width), fixed(width, head)],
        out_specs=moving(big, head),
        out_shape=jax.ShapeDtypeStruct((rows, head), BF16),
        name="input",
    )(tokens, gain_row, w_input)

    half_rows = rows // 2
    steps = half_rows // BLOCK
    state_shape = jax.ShapeDtypeStruct((2, rows, head // 2), F32)

    def recur(first, *extra):
        at = 0 if first else steps
        specs = [
            moving(BLOCK, head, at), fixed(4, head), fixed(1, head, head), fixed(1, head, head), fixed(1, head),
            pl.BlockSpec((1, BLOCK), lambda i: (0, i + at)),
        ]
        if first:
            specs += [fixed(16, width), fixed(1, width), fixed(width, head)]
        else:
            specs += [
                pl.BlockSpec((16, head), lambda i: (half_rows // 16 - 1, 0)),
                pl.BlockSpec((1, 8, head), lambda i: (0, 0, 0)), hbm, hbm,
            ]
        many = 1 if first else spans
        return pl.pallas_call(
            functools.partial(recur_kernel, first=first),
            grid=(steps,),
            in_specs=specs,
            out_specs=[halves(BLOCK, at), halves(BLOCK, at), fixed(many, 8, head)],
            out_shape=[state_shape, state_shape, jax.ShapeDtypeStruct((many, 8, head), F32)],
            scratch_shapes=[
                pltpu.VMEM((BLOCK + 8, head), F32), pltpu.VMEM((2, BLOCK, head // 2), F32),
                pltpu.VMEM((2, BLOCK, head // 2), F32), pltpu.VMEM((8, head), F32),
            ],
            input_output_aliases={} if first else {8: 0, 9: 1},
            name="recur",
        )(projected, conv_taps, w_rate, w_inlet, soft, decay_bias, *extra)

    state, prod, begun = recur(True, halo, gain_row, w_input)
    begun = advance(begun)
    state, prod, ends = recur(False, projected, begun, state, prod)
    all_ends = lax.all_to_all(ends, "sp", split_axis=0, concat_axis=0, tiled=True)
    gate_tokens = advance(tokens)
    gate_tokens, _ = tie(gate_tokens, ends)
    gate = pl.pallas_call(
        gate_kernel,
        grid=(rows // big,),
        in_specs=[moving(big, width), fixed(1, width), fixed(width, head)],
        out_specs=moving(big, head),
        out_shape=jax.ShapeDtypeStruct((rows, head), F32),
        name="gate",
    )(gate_tokens, gain_row, w_gate)
    gate = advance(gate)

    sent = pl.pallas_call(
        gated_kernel,
        grid=(heads // 2,),
        in_specs=[halves(big, 0), halves(big, 0), moving(big, head), fixed(spans, 8, head), fixed(1, head)],
        out_specs=pl.BlockSpec((2, 2, BLOCK + EXTRA, head // 2), lambda i: (i, 0, 0, 0)),
        out_shape=jax.ShapeDtypeStruct((heads, 2, BLOCK + EXTRA, head // 2), BF16),
        scratch_shapes=[pltpu.VMEM((8, head), F32)],
        name="gated",
    )(state, prod, gate, all_ends, out_gain.reshape(1, head))
    arrived = lax.all_to_all(sent, "tp", split_axis=0, concat_axis=0, tiled=True)
    holding = sent
    while len(moved) < reach - 2:
        holding = advance(holding)
    arrived = arrived.reshape(2 * heads, BLOCK + EXTRA, head // 2)
    arrived = advance(arrived)
    done = len(swapped) - 1
    offsets = [0] + [-k for k in range(1, done + 1)] + list(range(1, done + 1))
    sums = pl.pallas_call(
        functools.partial(early_kernel, offsets=offsets, spans=spans),
        in_specs=[vmem] * (2 + 2 * done),
        out_specs=vmem,
        out_shape=jax.ShapeDtypeStruct((BLOCK, out_width), F32),
        name="early",
    )(arrived, w_out, *moved[:done], *swapped[:done])
    while len(moved) < reach:
        sums = advance(sums)
    offsets = [-k for k in range(done + 1, reach + 1)] + list(range(done + 1, reach))
    return pl.pallas_call(
        functools.partial(late_kernel, offsets=offsets, spans=spans, channels=heads * head),
        in_specs=[vmem] * (2 + len(offsets)),
        out_specs=vmem,
        out_shape=jax.ShapeDtypeStruct((BLOCK, out_width), BF16),
        name="late",
    )(arrived, sums, *moved[done:], *swapped[done:])


def solution(mesh):
    return jax.shard_map(
        body,
        mesh=mesh,
        in_specs=(
            P(("grp", "sp"), None), P(), P(None, "tp"), P(None, "tp"), P(None, "tp"),
            P("tp", None, None), P("tp", None, None), P("tp"), P("tp", ("grp", "sp")), P("tp"), P("sp", None),
        ),
        out_specs=P(("grp", "sp", "tp"), None),
        check_vma=False,
    )
```

```python
import functools

import jax
import jax.numpy as jnp
from jax import lax
from jax.experimental import pallas as pl
from jax.experimental.pallas import tpu as pltpu
from jax.sharding import PartitionSpec as P

F32 = jnp.float32
BF16 = jnp.bfloat16
BLOCK = 256
SEG = 8
EXTRA = 16
EPS = 1e-06
STREAMS = 2
EXCHANGE = (2, 1, 3, 0)


def on_chip(x):
    return pltpu.with_memory_space_constraint(x, pltpu.VMEM)


def limit(mebibytes):
    return pltpu.CompilerParams(vmem_limit_bytes=mebibytes << 20)


def inverse_norm(rows):
    wide = rows.astype(F32)
    return lax.rsqrt(jnp.mean(wide * wide, axis=1, keepdims=True) + EPS)


def thirds(x):
    top = x.astype(BF16)
    rest = x - top.astype(F32)
    middle = rest.astype(BF16)
    return [top, middle, (rest - middle.astype(F32)).astype(BF16)]


def as_column(row, width):
    pieces = thirds(row) + [jnp.zeros((13, row.shape[1]), BF16)]
    return lax.dot_general(
        jnp.concatenate(pieces, 0), jnp.ones((16, width), BF16), (((0,), (0,)), ((), ())),
        preferred_element_type=F32,
    )


def softplus(x):
    e = jnp.exp(-jnp.abs(x))
    series = 1.0 / 6.0 - e * (1.0 / 7.0)
    for k in (5, 4, 3, 2):
        series = 1.0 / k - e * series
    small = e * (1.0 - e * series)
    return jnp.maximum(x, 0.0) + jnp.where(e < 0.06, small, jnp.log(1.0 + e))


def minus_expm1(y, exp_y):
    series = 1.0 / 120.0 + y * (1.0 / 720.0)
    series = 1.0 / 24.0 + y * series
    series = 1.0 / 6.0 + y * series
    series = 0.5 + y * series
    series = -y * (1.0 + y * series)
    return jnp.where(y > -0.25, series, 1.0 - exp_y)


def gelu(x):
    inner = 0.7978845608028654 * (x + 0.044715 * (x * x * x))
    return 0.5 * x * (1.0 + jnp.tanh(inner))


def logistic(x):
    return 1.0 / (1.0 + jnp.exp(-x))


def shifted_down(x, by, fill):
    rows = lax.broadcasted_iota(jnp.int32, x.shape, 0)
    return jnp.where(rows < by, fill, pltpu.roll(x, by, 0))


def branch_product(rows, weights):
    product = jnp.dot(rows, weights, preferred_element_type=F32)
    return (product * inverse_norm(rows)).astype(BF16)


def scaled_weights(weights, gain):
    return (weights[...].astype(F32) * as_column(gain[...], weights.shape[1])).astype(BF16)


def chunk_copy(source, target, sems, k):
    chunk = source.shape[0] // sems.shape[0]
    at = pl.ds(pl.multiple_of(k * chunk, chunk), chunk)
    return at, pltpu.make_async_copy(source.at[at, :], target.at[at, :], sems.at[k])


def input_kernel(tokens, gain, w_input, projected, scaled, kept, sems):
    count = sems.shape[0]
    for k in range(count):
        chunk_copy(tokens, kept, sems, k)[1].start()
    scaled[...] = scaled_weights(w_input, gain)

    def part(k, _):
        at, copy = chunk_copy(tokens, kept, sems, k)
        copy.wait()
        projected[at, :] = branch_product(kept[at, :], scaled[...])
        return 0

    lax.fori_loop(0, count, part, 0)


def gate_kernel(tokens, gain, w_gate, gate, scaled, kept, made, sems, out_sems):
    count = sems.shape[0]
    for k in range(count):
        chunk_copy(tokens, kept, sems, k)[1].start()
    scaled[...] = scaled_weights(w_gate, gain)

    def part(k, _):
        at, copy = chunk_copy(tokens, kept, sems, k)
        copy.wait()
        made[at, :] = gelu(branch_product(kept[at, :], scaled[...]).astype(F32))
        chunk_copy(made, gate, out_sems, k)[1].start()
        return 0

    lax.fori_loop(0, count, part, 0)
    for k in range(count):
        chunk_copy(made, gate, out_sems, k)[1].wait()


def recur_kernel(projected, taps, w_rate, w_inlet, decay_param, bias, *refs, first):
    if first:
        halo, scaled, refs = *refs[:2], refs[2:]
    else:
        begun, refs = refs[0], refs[1:]
    state_out, prod_out, ends, conv_buf, decay_buf, drive_buf, carry, state, prod, sems = refs
    if first:
        conv_buf[0:8, :] = branch_product(halo[...], scaled[...]).astype(F32)[8:16]
        head_row = lax.broadcasted_iota(jnp.int32, carry.shape, 0) == 0
        carry[...] = jnp.where(head_row, 1.0, 0.0)
    else:
        middle = projected.shape[0] // 2
        conv_buf[0:8, :] = projected[middle - 16 : middle, :].astype(F32)[8:16]
        carry[...] = begun[0]
    soft = softplus(-decay_param[...])
    blocks = projected.shape[0] // 2 // BLOCK
    segs = BLOCK // SEG

    def leaving(k):
        at = (slice(None), pl.ds(pl.multiple_of(k * BLOCK, BLOCK), BLOCK), slice(None))
        return [
            pltpu.make_async_copy(ref.at[at], out.at[at], sems.at[n, k])
            for n, (ref, out) in enumerate(((state, state_out), (prod, prod_out)))
        ]

    def part(k, _):
        block = k + (0 if first else blocks)
        start = pl.multiple_of(block * BLOCK, BLOCK)
        conv_buf[8 : BLOCK + 8, :] = projected[pl.ds(start, BLOCK), :].astype(F32)
        summed = conv_buf[5 : BLOCK + 5, :] * taps[0:1, :]
        for tap in range(1, 4):
            summed = summed + conv_buf[5 + tap : BLOCK + 5 + tap, :] * taps[tap : tap + 1, :]
        conv_buf[0:8, :] = conv_buf[BLOCK : BLOCK + 8, :]
        convolved = summed.astype(BF16)
        rate = logistic(jnp.dot(convolved, w_rate[0], preferred_element_type=F32))
        inlet = logistic(jnp.dot(convolved, w_inlet[0], preferred_element_type=F32))
        log_decay = -8.0 * rate * soft + as_column(bias[0:1, pl.ds(start, BLOCK)], rate.shape[1])
        decay = jnp.exp(log_decay)
        drive = jnp.sqrt(minus_expm1(2.0 * log_decay, decay * decay)) * inlet * convolved.astype(F32)
        for half in range(2):
            lanes = slice(half * 128, half * 128 + 128)
            decay_buf[half] = decay[:, lanes]
            drive_buf[half] = drive[:, lanes]
            row = [(half, pl.ds(r, segs, stride=SEG), slice(None)) for r in range(SEG)]
            p, h = decay_buf[row[0]], drive_buf[row[0]]
            inner = [(p, h)]
            for r in range(1, SEG):
                a = decay_buf[row[r]]
                h = a * h + drive_buf[row[r]]
                p = a * p
                inner.append((p, h))
            by = 1
            while by < segs:
                h = h + p * shifted_down(h, by, 0.0)
                p = p * shifted_down(p, by, 1.0)
                by *= 2
            carry_p, carry_h = carry[0:1, lanes], carry[1:2, lanes]
            start_h = shifted_down(h, 1, 0.0) + shifted_down(p, 1, 1.0) * carry_h
            start_p = shifted_down(p, 1, 1.0) * carry_p
            carry[1:2, lanes] = h[segs - 1 : segs, :] + p[segs - 1 : segs, :] * carry_h
            carry[0:1, lanes] = p[segs - 1 : segs, :] * carry_p
            for r in range(SEG):
                p, h = inner[r]
                at = (half, pl.ds(pl.multiple_of(k * BLOCK, BLOCK) + r, segs, stride=SEG), slice(None))
                state[at] = h + p * start_h
                prod[at] = p * start_p
        for copy in leaving(k):
            copy.start()
        return 0

    lax.fori_loop(0, blocks, part, 0)
    for k in range(blocks):
        for copy in leaving(k):
            copy.wait()
    ends[...] = jnp.broadcast_to(carry[...][None], ends.shape)


def gated_kernel(state_1, state_2, prod_1, prod_2, gate, ends, gain, sent, incoming, states, prods, gates, sems):
    count = sent.shape[0]
    copies = []
    for d in range(count):
        state, prod = (state_1, prod_1) if d < count // 2 else (state_2, prod_2)
        near = pl.ds(d % (count // 2) * BLOCK, BLOCK)
        at = pl.ds(d * BLOCK, BLOCK)
        copies.append(
            [
                pltpu.make_async_copy(state.at[:, near, :], states.at[:, at, :], sems.at[0, d]),
                pltpu.make_async_copy(prod.at[:, near, :], prods.at[:, at, :], sems.at[1, d]),
                pltpu.make_async_copy(gate.at[at, :], gates.at[at, :], sems.at[2, d]),
            ]
        )
        for copy in copies[-1]:
            copy.start()
    span = lax.axis_index("sp")
    total = jnp.zeros((1, gain.shape[1]), F32)
    for k in range(ends.shape[0]):
        total = jnp.where(k < span, ends[k, 0:1, :] * total + ends[k, 1:2, :], total)
    incoming[...] = jnp.broadcast_to(total, incoming.shape)

    ones = jnp.ones((8, 128), BF16)
    over = (((1,), (1,)), ((), ()))
    for d in range(count):
        for copy in copies[d]:
            copy.wait()
        rows = slice(d * BLOCK, d * BLOCK + BLOCK)
        total = jnp.zeros((8, BLOCK), F32)
        for half in range(2):
            lanes = slice(half * 128, half * 128 + 128)
            gated = (states[half, rows, :] + prods[half, rows, :] * incoming[0:1, lanes]) * gates[rows, lanes]
            sent[d, half, 0:BLOCK, :] = (gated * gain[:, lanes]).astype(BF16)
            square = gated * gated
            high = square.astype(BF16)
            low = (square - high.astype(F32)).astype(BF16)
            total = total + lax.dot_general(ones, high, over, preferred_element_type=F32)
            total = total + lax.dot_general(ones, low, over, preferred_element_type=F32)
        top = total.astype(BF16).astype(F32)
        row = lax.broadcasted_iota(jnp.int32, total.shape, 0)
        lines = jnp.where(row == 0, top, jnp.where(row == 1, total - top, 0.0))
        lines = jnp.concatenate([lines, jnp.zeros_like(lines)], 0).astype(BF16)
        for half in range(2):
            sent[d, half, BLOCK : BLOCK + EXTRA, :] = lines[:, half * 128 : half * 128 + 128]


def product(arrived, places, blocks, low, step):
    mixed = jnp.concatenate([arrived[place, 0:BLOCK, :] for place in places], 1)
    weights = jnp.concatenate([block[:, low : low + step] for block in blocks], 0)
    return jnp.dot(mixed, weights, preferred_element_type=F32)


def places_of(offsets, spans):
    span, core = lax.axis_index("sp"), lax.axis_index("tp") % 2
    return [lax.rem(span + spans + jnp.where(core == 0, k, -k), spans) for k in offsets]


def joined(blocks, depth):
    whole, parts = [], []
    for block in blocks:
        parts.append(block)
        if sum(part.shape[0] for part in parts) == depth:
            whole.append(parts)
            parts = []
    return whole


def product(arrived, places, groups, low, step):
    mixed = jnp.concatenate([arrived[place, 0:BLOCK, :] for place in places], 1)
    weights = jnp.concatenate([part[:, low : low + step] for parts in groups for part in parts], 0)
    return jnp.dot(mixed, weights, preferred_element_type=F32)


def early_kernel(arrived, *refs, offsets, spans, depth):
    groups, out = joined(refs[:-1], depth), refs[-1]
    places = places_of(offsets, spans)
    step = 512
    for low in range(0, out.shape[1], step):
        out[:, low : low + step] = product(arrived, places, groups, low, step)


def late_kernel(arrived, sums, *refs, offsets, spans, depth, channels):
    groups, out = joined(refs[:-1], depth), refs[-1]
    places = places_of(offsets, spans)
    ones = jnp.ones((arrived.shape[0] // 2 * EXTRA, 128), BF16)
    square = []
    for half in range(2):
        lines = [arrived[k, BLOCK : BLOCK + EXTRA, :] for k in range(half, arrived.shape[0], 2)]
        square.append(
            lax.dot_general(
                jnp.concatenate(lines, 0), ones, (((0,), (0,)), ((), ())), preferred_element_type=F32
            )
        )
    scale = lax.rsqrt(jnp.concatenate(square, 0)[:, 0:1] / channels + EPS)
    step = 512
    for low in range(0, out.shape[1], step):
        acc = sums[:, low : low + step] + product(arrived, places, groups, low, step)
        out[:, low : low + step] = (acc * scale).astype(BF16)


def tie(*values):
    return lax.optimization_barrier(values)


def body(
    tokens, in_gain, w_input, w_gate, conv_taps, w_rate, w_inlet, decay_param, decay_bias, out_gain, w_out
):
    rows, width = tokens.shape
    head = w_input.shape[1]
    spans, heads = lax.axis_size("sp"), lax.axis_size("tp")
    depth, out_width = w_out.shape
    reach = spans // 2

    around = []
    swap = []
    for z in range(spans):
        for t in range(heads):
            ahead = (z + 1) % spans if t % 2 == 0 else (z - 1) % spans
            around.append((z * heads + t, ahead * heads + t))
            swap.append((z * heads + t, z * heads + t + 1 - 2 * (t % 2)))

    moved, swapped = [], []

    def onward(parts):
        moved.append([lax.ppermute(part, ("sp", "tp"), around) for part in parts])

    def across(parts):
        swapped.append([lax.ppermute(part, ("sp", "tp"), swap) for part in parts])

    def advance(value, pieces=1):
        before = swapped[-1] if swapped else []
        value, *rest = tie(value, *before, *moved[-1][:1])
        if swapped:
            swapped[-1] = rest[:-1]
        moved[-1] = rest[-1:] + moved[-1][1:]
        if len(moved) < reach:
            parts = moved[-1]
            if len(parts) < pieces:
                cut = depth // pieces
                parts = [parts[0][k * cut : k * cut + cut] for k in range(pieces)]
            onward(parts)
            across(moved[-2])
        return value

    fixed = pl.BlockSpec(memory_space=pltpu.VMEM)
    hbm = pl.BlockSpec(memory_space=pltpu.HBM)
    onward([w_out])
    halo = lax.ppermute(tokens[rows - 16 :], "sp", [(i, i + 1) for i in range(spans - 1)])
    gain_row = in_gain.reshape(1, width)

    in_hbm = lambda x: pltpu.with_memory_space_constraint(x, pltpu.HBM)
    projected, scaled = pl.pallas_call(
        input_kernel,
        in_specs=[hbm, fixed, fixed],
        out_specs=[fixed] * 2,
        out_shape=[pltpu.VMEM((rows, head), BF16), pltpu.VMEM((width, head), BF16)],
        scratch_shapes=[pltpu.VMEM((rows, width), BF16), pltpu.SemaphoreType.DMA((4,))],
        compiler_params=limit(16),
        name="input",
    )(in_hbm(tokens), gain_row, w_input)

    half_rows = rows // 2

    def recur(first, *extra):
        many = 1 if first else spans
        half_shape = (2, half_rows, head // 2)
        return pl.pallas_call(
            functools.partial(recur_kernel, first=first),
            in_specs=[fixed] * (6 + len(extra)),
            out_specs=[hbm, hbm, fixed],
            out_shape=[
                pltpu.HBM(half_shape, F32), pltpu.HBM(half_shape, F32),
                jax.ShapeDtypeStruct((many, 8, head), F32),
            ],
            scratch_shapes=[
                pltpu.VMEM((BLOCK + 8, head), F32), pltpu.VMEM((2, BLOCK, head // 2), F32),
                pltpu.VMEM((2, BLOCK, head // 2), F32), pltpu.VMEM((8, head), F32),
                pltpu.VMEM(half_shape, F32), pltpu.VMEM(half_shape, F32),
                pltpu.SemaphoreType.DMA((2, half_rows // BLOCK)),
            ],
            compiler_params=limit(12),
            name="recur",
        )(on_chip(projected), conv_taps, w_rate, w_inlet, decay_param.reshape(1, head), decay_bias, *extra)

    projected = advance(projected)
    state_1, prod_1, begun = recur(True, halo, on_chip(scaled))
    state_2, prod_2, ends = recur(False, begun)
    ends = advance(ends)
    all_ends = lax.all_to_all(ends, "sp", split_axis=0, concat_axis=0, tiled=True)
    late_tokens, _ = tie(tokens, ends)
    gate = pl.pallas_call(
        gate_kernel,
        in_specs=[hbm, fixed, fixed],
        out_specs=hbm,
        out_shape=pltpu.HBM((rows, head), F32),
        scratch_shapes=[
            pltpu.VMEM((width, head), BF16), pltpu.VMEM((rows, width), BF16), pltpu.VMEM((rows, head), F32),
            pltpu.SemaphoreType.DMA((4,)), pltpu.SemaphoreType.DMA((4,)),
        ],
        compiler_params=limit(20),
        name="gate",
    )(in_hbm(late_tokens), gain_row, w_gate)
    gate = advance(gate)

    sent = pl.pallas_call(
        gated_kernel,
        in_specs=[hbm] * 5 + [fixed] * 2,
        out_specs=fixed,
        out_shape=pltpu.VMEM((heads, 2, BLOCK + EXTRA, head // 2), BF16),
        scratch_shapes=[
            pltpu.VMEM((8, head), F32), pltpu.VMEM((2, rows, head // 2), F32),
            pltpu.VMEM((2, rows, head // 2), F32), pltpu.VMEM((rows, head), F32),
            pltpu.SemaphoreType.DMA((3, heads)),
        ],
        compiler_params=limit(12),
        name="gated",
    )(*map(in_hbm, (state_1, state_2, prod_1, prod_2, gate)), all_ends, out_gain.reshape(1, head))
    seat = lax.axis_index("tp")
    chips = heads // 2
    arrived = lax.dynamic_slice_in_dim(sent, seat, 1, 0)
    arrived = lax.dynamic_update_slice_in_dim(jnp.zeros_like(sent), arrived, seat, 0)
    order = [(dx, dc) for dx in EXCHANGE for dc in range(2) if (dx, dc) != (0, 0)]
    moves = []
    for dx, dc in order:
        to = lambda t: (t // 2 + dx) % chips * 2 + (t % 2 + dc) % 2
        part = lax.dynamic_slice_in_dim(sent, to(seat), 1, 0)
        moves.append(lax.ppermute(part, "tp", [(t, to(t)) for t in range(heads)]))
    for (dx, dc), part in zip(order, moves):
        source = (seat // 2 - dx + chips) % chips * 2 + (seat % 2 + dc) % 2
        arrived = lax.dynamic_update_slice_in_dim(arrived, part, source, 0)
    holding = sent
    while len(moved) < reach - 2:
        holding = advance(holding, STREAMS)
    arrived = arrived.reshape(2 * heads, BLOCK + EXTRA, head // 2)
    arrived = advance(arrived, STREAMS)
    flat = lambda groups: [on_chip(part) for parts in groups for part in parts]
    done = len(swapped) - 1
    offsets = [0] + [-k for k in range(1, done + 1)] + list(range(1, done + 1))
    blocks = [on_chip(w_out)] + flat(moved[:done]) + flat(swapped[:done])
    sums = pl.pallas_call(
        functools.partial(early_kernel, offsets=offsets, spans=spans, depth=depth),
        in_specs=[fixed] * (1 + len(blocks)),
        out_specs=fixed,
        out_shape=pltpu.VMEM((BLOCK, out_width), F32),
        compiler_params=limit(16),
        name="early",
    )(arrived, *blocks)
    while len(moved) < reach:
        sums = advance(sums, STREAMS)
    offsets = [-k for k in range(done + 1, reach + 1)] + list(range(done + 1, reach))
    blocks = flat(moved[done:]) + flat(swapped[done:])
    return pl.pallas_call(
        functools.partial(late_kernel, offsets=offsets, spans=spans, depth=depth, channels=heads * head),
        in_specs=[fixed] * (2 + len(blocks)),
        out_specs=fixed,
        out_shape=jax.ShapeDtypeStruct((BLOCK, out_width), BF16),
        compiler_params=limit(16),
        name="late",
    )(arrived, on_chip(sums), *blocks)


def solution(mesh):
    return jax.shard_map(
        body,
        mesh=mesh,
        in_specs=(
            P(("grp", "sp"), None), P(), P(None, "tp"), P(None, "tp"), P(None, "tp"),
            P("tp", None, None), P("tp", None, None), P("tp"), P("tp", ("grp", "sp")), P("tp"), P("sp", None),
        ),
        out_specs=P(("grp", "sp", "tp"), None),
        check_vma=False,
    )
```

```python
import functools

import jax
import jax.numpy as jnp
from jax import lax
from jax.experimental import pallas as pl
from jax.experimental.pallas import tpu as pltpu
from jax.sharding import PartitionSpec as P

F32 = jnp.float32
BF16 = jnp.bfloat16
BLOCK = 256
SEG = 8
EXTRA = 16
EPS = 1e-06
STREAMS = 2
EXCHANGE = (2, 1, 3, 0)


def on_chip(x):
    return pltpu.with_memory_space_constraint(x, pltpu.VMEM)


def limit(mebibytes):
    return pltpu.CompilerParams(vmem_limit_bytes=mebibytes << 20)


def inverse_norm(rows):
    wide = rows.astype(F32)
    return lax.rsqrt(jnp.mean(wide * wide, axis=1, keepdims=True) + EPS)


def thirds(x):
    top = x.astype(BF16)
    rest = x - top.astype(F32)
    middle = rest.astype(BF16)
    return [top, middle, (rest - middle.astype(F32)).astype(BF16)]


def as_column(row, width):
    pieces = thirds(row) + [jnp.zeros((13, row.shape[1]), BF16)]
    return lax.dot_general(
        jnp.concatenate(pieces, 0), jnp.ones((16, width), BF16), (((0,), (0,)), ((), ())),
        preferred_element_type=F32,
    )


def softplus(x):
    e = jnp.exp(-jnp.abs(x))
    series = 1.0 / 6.0 - e * (1.0 / 7.0)
    for k in (5, 4, 3, 2):
        series = 1.0 / k - e * series
    small = e * (1.0 - e * series)
    return jnp.maximum(x, 0.0) + jnp.where(e < 0.06, small, jnp.log(1.0 + e))


def minus_expm1(y, exp_y):
    series = 1.0 / 120.0 + y * (1.0 / 720.0)
    series = 1.0 / 24.0 + y * series
    series = 1.0 / 6.0 + y * series
    series = 0.5 + y * series
    series = -y * (1.0 + y * series)
    return jnp.where(y > -0.25, series, 1.0 - exp_y)


def gelu(x):
    inner = 0.7978845608028654 * (x + 0.044715 * (x * x * x))
    return 0.5 * x * (1.0 + jnp.tanh(inner))


def logistic(x):
    return 1.0 / (1.0 + jnp.exp(-x))


def shifted_down(x, by, fill):
    rows = lax.broadcasted_iota(jnp.int32, x.shape, 0)
    return jnp.where(rows < by, fill, pltpu.roll(x, by, 0))


def branch_product(rows, weights):
    product = jnp.dot(rows, weights, preferred_element_type=F32)
    return (product * inverse_norm(rows)).astype(BF16)


def scaled_weights(weights, gain):
    return (weights[...].astype(F32) * as_column(gain[...], weights.shape[1])).astype(BF16)


def chunk_copy(source, target, sems, k):
    chunk = source.shape[0] // sems.shape[0]
    at = pl.ds(pl.multiple_of(k * chunk, chunk), chunk)
    return at, pltpu.make_async_copy(source.at[at, :], target.at[at, :], sems.at[k])


def input_kernel(tokens, gain, w_input, projected, scaled, kept, gain_here, w_here, sems, small_sems):
    count = sems.shape[0]
    small = [
        pltpu.make_async_copy(gain, gain_here, small_sems.at[0]),
        pltpu.make_async_copy(w_input, w_here, small_sems.at[1]),
    ]
    for copy in small:
        copy.start()
    for k in range(count):
        chunk_copy(tokens, kept, sems, k)[1].start()
    for copy in small:
        copy.wait()
    scaled[...] = scaled_weights(w_here, gain_here)

    def part(k, _):
        at, copy = chunk_copy(tokens, kept, sems, k)
        copy.wait()
        projected[at, :] = branch_product(kept[at, :], scaled[...])
        return 0

    lax.fori_loop(0, count, part, 0)


def gate_kernel(tokens, gain, w_gate, gate, scaled, kept, made, sems, out_sems):
    count = sems.shape[0]
    for k in range(count):
        chunk_copy(tokens, kept, sems, k)[1].start()
    scaled[...] = scaled_weights(w_gate, gain)

    def part(k, _):
        at, copy = chunk_copy(tokens, kept, sems, k)
        copy.wait()
        made[at, :] = gelu(branch_product(kept[at, :], scaled[...]).astype(F32))
        chunk_copy(made, gate, out_sems, k)[1].start()
        return 0

    lax.fori_loop(0, count, part, 0)
    for k in range(count):
        chunk_copy(made, gate, out_sems, k)[1].wait()


def recur_kernel(projected, taps, w_rate, w_inlet, decay_param, bias, *refs, first):
    if first:
        halo, scaled, refs = *refs[:2], refs[2:]
    else:
        begun, refs = refs[0], refs[1:]
    state_out, prod_out, ends, conv_buf, decay_buf, drive_buf, carry, state, prod, sems = refs
    if first:
        conv_buf[0:8, :] = branch_product(halo[...], scaled[...]).astype(F32)[8:16]
        head_row = lax.broadcasted_iota(jnp.int32, carry.shape, 0) == 0
        carry[...] = jnp.where(head_row, 1.0, 0.0)
    else:
        middle = projected.shape[0] // 2
        conv_buf[0:8, :] = projected[middle - 16 : middle, :].astype(F32)[8:16]
        carry[...] = begun[0]
    soft = softplus(-decay_param[...])
    blocks = projected.shape[0] // 2 // BLOCK
    segs = BLOCK // SEG

    def leaving(k):
        at = (slice(None), pl.ds(pl.multiple_of(k * BLOCK, BLOCK), BLOCK), slice(None))
        return [
            pltpu.make_async_copy(ref.at[at], out.at[at], sems.at[n, k])
            for n, (ref, out) in enumerate(((state, state_out), (prod, prod_out)))
        ]

    def part(k, _):
        block = k + (0 if first else blocks)
        start = pl.multiple_of(block * BLOCK, BLOCK)
        conv_buf[8 : BLOCK + 8, :] = projected[pl.ds(start, BLOCK), :].astype(F32)
        summed = conv_buf[5 : BLOCK + 5, :] * taps[0:1, :]
        for tap in range(1, 4):
            summed = summed + conv_buf[5 + tap : BLOCK + 5 + tap, :] * taps[tap : tap + 1, :]
        conv_buf[0:8, :] = conv_buf[BLOCK : BLOCK + 8, :]
        convolved = summed.astype(BF16)
        rate = logistic(jnp.dot(convolved, w_rate[0], preferred_element_type=F32))
        inlet = logistic(jnp.dot(convolved, w_inlet[0], preferred_element_type=F32))
        log_decay = -8.0 * rate * soft + as_column(bias[0:1, pl.ds(start, BLOCK)], rate.shape[1])
        decay = jnp.exp(log_decay)
        drive = jnp.sqrt(minus_expm1(2.0 * log_decay, decay * decay)) * inlet * convolved.astype(F32)
        for half in range(2):
            lanes = slice(half * 128, half * 128 + 128)
            decay_buf[half] = decay[:, lanes]
            drive_buf[half] = drive[:, lanes]
            row = [(half, pl.ds(r, segs, stride=SEG), slice(None)) for r in range(SEG)]
            p, h = decay_buf[row[0]], drive_buf[row[0]]
            inner = [(p, h)]
            for r in range(1, SEG):
                a = decay_buf[row[r]]
                h = a * h + drive_buf[row[r]]
                p = a * p
                inner.append((p, h))
            by = 1
            while by < segs:
                h = h + p * shifted_down(h, by, 0.0)
                p = p * shifted_down(p, by, 1.0)
                by *= 2
            carry_p, carry_h = carry[0:1, lanes], carry[1:2, lanes]
            start_h = shifted_down(h, 1, 0.0) + shifted_down(p, 1, 1.0) * carry_h
            start_p = shifted_down(p, 1, 1.0) * carry_p
            carry[1:2, lanes] = h[segs - 1 : segs, :] + p[segs - 1 : segs, :] * carry_h
            carry[0:1, lanes] = p[segs - 1 : segs, :] * carry_p
            for r in range(SEG):
                p, h = inner[r]
                at = (half, pl.ds(pl.multiple_of(k * BLOCK, BLOCK) + r, segs, stride=SEG), slice(None))
                state[at] = h + p * start_h
                prod[at] = p * start_p
        for copy in leaving(k):
            copy.start()
        return 0

    lax.fori_loop(0, blocks, part, 0)
    for k in range(blocks):
        for copy in leaving(k):
            copy.wait()
    ends[...] = jnp.broadcast_to(carry[...][None], ends.shape)


def gated_kernel(state_1, state_2, prod_1, prod_2, gate, ends, gain, sent, incoming, states, prods, gates, sems):
    count = sent.shape[0]
    copies = []
    for d in range(count):
        state, prod = (state_1, prod_1) if d < count // 2 else (state_2, prod_2)
        near = pl.ds(d % (count // 2) * BLOCK, BLOCK)
        at = pl.ds(d * BLOCK, BLOCK)
        copies.append(
            [
                pltpu.make_async_copy(state.at[:, near, :], states.at[:, at, :], sems.at[0, d]),
                pltpu.make_async_copy(prod.at[:, near, :], prods.at[:, at, :], sems.at[1, d]),
                pltpu.make_async_copy(gate.at[at, :], gates.at[at, :], sems.at[2, d]),
            ]
        )
        for copy in copies[-1]:
            copy.start()
    span = lax.axis_index("sp")
    total = jnp.zeros((1, gain.shape[1]), F32)
    for k in range(ends.shape[0]):
        total = jnp.where(k < span, ends[k, 0:1, :] * total + ends[k, 1:2, :], total)
    incoming[...] = jnp.broadcast_to(total, incoming.shape)

    ones = jnp.ones((8, 128), BF16)
    over = (((1,), (1,)), ((), ()))
    for d in range(count):
        for copy in copies[d]:
            copy.wait()
        rows = slice(d * BLOCK, d * BLOCK + BLOCK)
        total = jnp.zeros((8, BLOCK), F32)
        for half in range(2):
            lanes = slice(half * 128, half * 128 + 128)
            gated = (states[half, rows, :] + prods[half, rows, :] * incoming[0:1, lanes]) * gates[rows, lanes]
            sent[d, half, 0:BLOCK, :] = (gated * gain[:, lanes]).astype(BF16)
            square = gated * gated
            high = square.astype(BF16)
            low = (square - high.astype(F32)).astype(BF16)
            total = total + lax.dot_general(ones, high, over, preferred_element_type=F32)
            total = total + lax.dot_general(ones, low, over, preferred_element_type=F32)
        top = total.astype(BF16).astype(F32)
        row = lax.broadcasted_iota(jnp.int32, total.shape, 0)
        lines = jnp.where(row == 0, top, jnp.where(row == 1, total - top, 0.0))
        lines = jnp.concatenate([lines, jnp.zeros_like(lines)], 0).astype(BF16)
        for half in range(2):
            sent[d, half, BLOCK : BLOCK + EXTRA, :] = lines[:, half * 128 : half * 128 + 128]


def neighbour(seat, dx, dc, chips):
    return lax_rem(seat // 2 + dx, chips) * 2 + lax_rem(seat % 2 + dc, 2)


def lax_rem(a, b):
    return a % b if isinstance(a, int) else lax.rem(a, b)


def places_of(offsets, spans):
    span, core = lax.axis_index("sp"), lax.axis_index("tp") % 2
    return [lax.rem(span + spans + jnp.where(core == 0, k, -k), spans) for k in offsets]


def joined(blocks, depth):
    whole, parts = [], []
    for block in blocks:
        parts.append(block)
        if sum(part.shape[0] for part in parts) == depth:
            whole.append(parts)
            parts = []
    return whole


def product(arrived, places, groups, low, step):
    mixed = jnp.concatenate([arrived[lax.div(place, 2), lax.rem(place, 2), 0:BLOCK, :] for place in places], 1)
    weights = jnp.concatenate([part[:, low : low + step] for parts in groups for part in parts], 0)
    return jnp.dot(mixed, weights, preferred_element_type=F32)


def early_kernel(*refs, order, offsets, spans, depth):
    count = len(order)
    out, arrived = refs[-2:]
    seat = lax.axis_index("tp")
    for (dx, dc), part in zip(order, refs[:count]):
        arrived[neighbour(seat, count // 2 - dx, dc, count // 2)] = part[0]
    groups = joined(refs[count:-2], depth)
    places = places_of(offsets, spans)
    step = 512
    for low in range(0, out.shape[1], step):
        out[:, low : low + step] = product(arrived, places, groups, low, step)


def late_kernel(arrived, sums, *refs, offsets, spans, depth, channels):
    groups, out = joined(refs[:-1], depth), refs[-1]
    places = places_of(offsets, spans)
    ones = jnp.ones((arrived.shape[0] * EXTRA, 128), BF16)
    square = []
    for half in range(2):
        lines = [arrived[k, half, BLOCK : BLOCK + EXTRA, :] for k in range(arrived.shape[0])]
        square.append(
            lax.dot_general(
                jnp.concatenate(lines, 0), ones, (((0,), (0,)), ((), ())), preferred_element_type=F32
            )
        )
    scale = lax.rsqrt(jnp.concatenate(square, 0)[:, 0:1] / channels + EPS)
    step = 512
    for low in range(0, out.shape[1], step):
        acc = sums[:, low : low + step] + product(arrived, places, groups, low, step)
        out[:, low : low + step] = (acc * scale).astype(BF16)


def tie(*values):
    return lax.optimization_barrier(values)


def body(
    tokens, in_gain, w_input, w_gate, conv_taps, w_rate, w_inlet, decay_param, decay_bias, out_gain, w_out
):
    rows, width = tokens.shape
    head = w_input.shape[1]
    spans, heads = lax.axis_size("sp"), lax.axis_size("tp")
    depth, out_width = w_out.shape
    reach = spans // 2

    around = []
    swap = []
    for z in range(spans):
        for t in range(heads):
            ahead = (z + 1) % spans if t % 2 == 0 else (z - 1) % spans
            around.append((z * heads + t, ahead * heads + t))
            swap.append((z * heads + t, z * heads + t + 1 - 2 * (t % 2)))

    moved, swapped = [], []

    def onward(parts):
        made = []
        for part in parts:
            made.append(lax.ppermute(part, ("sp", "tp"), around))
        moved.append(made)

    def across(parts):
        made = []
        for part in parts:
            made.append(lax.ppermute(part, ("sp", "tp"), swap))
        swapped.append(made)

    def advance(value, pieces=1):
        before = swapped[-2] if len(swapped) > 1 else []
        value, *rest = tie(value, *before, *moved[-1][:1])
        if before:
            swapped[-2] = rest[:-1]
        moved[-1] = rest[-1:] + moved[-1][1:]
        if len(moved) < reach:
            parts = moved[-1]
            if len(parts) < pieces:
                cut = depth // pieces
                parts = [parts[0][k * cut : k * cut + cut] for k in range(pieces)]
            onward(parts)
            across(moved[-2])
        return value

    fixed = pl.BlockSpec(memory_space=pltpu.VMEM)
    hbm = pl.BlockSpec(memory_space=pltpu.HBM)
    onward([w_out])
    halo = lax.ppermute(tokens[rows - 16 :], "sp", [(i, i + 1) for i in range(spans - 1)])
    gain_row = in_gain.reshape(1, width)

    in_hbm = lambda x: pltpu.with_memory_space_constraint(x, pltpu.HBM)
    projected, scaled = pl.pallas_call(
        input_kernel,
        in_specs=[hbm] * 3,
        out_specs=[fixed] * 2,
        out_shape=[pltpu.VMEM((rows, head), BF16), pltpu.VMEM((width, head), BF16)],
        scratch_shapes=[
            pltpu.VMEM((rows, width), BF16), pltpu.VMEM((1, width), F32), pltpu.VMEM((width, head), BF16),
            pltpu.SemaphoreType.DMA((4,)), pltpu.SemaphoreType.DMA((2,)),
        ],
        compiler_params=limit(16),
        name="input",
    )(in_hbm(tokens), in_hbm(gain_row), in_hbm(w_input))

    half_rows = rows // 2

    def recur(first, *extra):
        many = 1 if first else spans
        half_shape = (2, half_rows, head // 2)
        return pl.pallas_call(
            functools.partial(recur_kernel, first=first),
            in_specs=[fixed] * (6 + len(extra)),
            out_specs=[hbm, hbm, fixed],
            out_shape=[
                pltpu.HBM(half_shape, F32), pltpu.HBM(half_shape, F32),
                jax.ShapeDtypeStruct((many, 8, head), F32),
            ],
            scratch_shapes=[
                pltpu.VMEM((BLOCK + 8, head), F32), pltpu.VMEM((2, BLOCK, head // 2), F32),
                pltpu.VMEM((2, BLOCK, head // 2), F32), pltpu.VMEM((8, head), F32),
                pltpu.VMEM(half_shape, F32), pltpu.VMEM(half_shape, F32),
                pltpu.SemaphoreType.DMA((2, half_rows // BLOCK)),
            ],
            compiler_params=limit(12),
            name="recur",
        )(on_chip(projected), conv_taps, w_rate, w_inlet, decay_param.reshape(1, head), decay_bias, *extra)

    projected = advance(projected)
    state_1, prod_1, begun = recur(True, halo, on_chip(scaled))
    state_2, prod_2, ends = recur(False, begun)
    ends = advance(ends)
    all_ends = lax.all_to_all(ends, "sp", split_axis=0, concat_axis=0, tiled=True)
    late_tokens, _ = tie(tokens, ends)
    gate = pl.pallas_call(
        gate_kernel,
        in_specs=[hbm, fixed, fixed],
        out_specs=hbm,
        out_shape=pltpu.HBM((rows, head), F32),
        scratch_shapes=[
            pltpu.VMEM((width, head), BF16), pltpu.VMEM((rows, width), BF16), pltpu.VMEM((rows, head), F32),
            pltpu.SemaphoreType.DMA((4,)), pltpu.SemaphoreType.DMA((4,)),
        ],
        compiler_params=limit(20),
        name="gate",
    )(in_hbm(late_tokens), gain_row, w_gate)
    gate = advance(gate)

    sent = pl.pallas_call(
        gated_kernel,
        in_specs=[hbm] * 5 + [fixed] * 2,
        out_specs=fixed,
        out_shape=pltpu.VMEM((heads, 2, BLOCK + EXTRA, head // 2), BF16),
        scratch_shapes=[
            pltpu.VMEM((8, head), F32), pltpu.VMEM((2, rows, head // 2), F32),
            pltpu.VMEM((2, rows, head // 2), F32), pltpu.VMEM((rows, head), F32),
            pltpu.SemaphoreType.DMA((3, heads)),
        ],
        compiler_params=limit(12),
        name="gated",
    )(*map(in_hbm, (state_1, state_2, prod_1, prod_2, gate)), all_ends, out_gain.reshape(1, head))
    seat = lax.axis_index("tp")
    order = [(dx, dc) for dx in EXCHANGE for dc in range(2) if (dx, dc) != (0, 0)]
    moves = []
    for dx, dc in order:
        to = lambda t: neighbour(t, dx, dc, heads // 2)
        if (dx, dc) == (1, 0):
            sent = advance(sent, STREAMS)
        part = lax.dynamic_slice_in_dim(sent, to(seat), 1, 0)
        moves.append(lax.ppermute(part, "tp", [(t, to(t)) for t in range(heads)]))
    holding = sent
    while len(moved) < reach - 1:
        holding = advance(holding, STREAMS)
    own = lax.dynamic_slice_in_dim(holding, seat, 1, 0)
    flat = lambda groups: [on_chip(part) for parts in groups for part in parts]
    done = len(swapped) - 1
    offsets = [0] + [-k for k in range(1, done + 1)] + list(range(1, done + 1))
    blocks = [on_chip(w_out)] + flat(moved[:done]) + flat(swapped[:done])
    sums, arrived = pl.pallas_call(
        functools.partial(early_kernel, order=[(0, 0)] + order, offsets=offsets, spans=spans, depth=depth),
        in_specs=[fixed] * (1 + len(moves) + len(blocks)),
        out_specs=[fixed] * 2,
        out_shape=[pltpu.VMEM((BLOCK, out_width), F32), pltpu.VMEM(sent.shape, BF16)],
        compiler_params=limit(12),
        name="early",
    )(on_chip(own), *map(on_chip, moves), *blocks)
    while len(moved) < reach:
        sums = advance(sums, STREAMS)
    offsets = [-k for k in range(done + 1, reach + 1)] + list(range(done + 1, reach))
    blocks = flat(moved[done:]) + flat(swapped[done:])
    return pl.pallas_call(
        functools.partial(late_kernel, offsets=offsets, spans=spans, depth=depth, channels=heads * head),
        in_specs=[fixed] * (2 + len(blocks)),
        out_specs=fixed,
        out_shape=jax.ShapeDtypeStruct((BLOCK, out_width), BF16),
        compiler_params=limit(12),
        name="late",
    )(on_chip(arrived), on_chip(sums), *blocks)


def solution(mesh):
    return jax.shard_map(
        body,
        mesh=mesh,
        in_specs=(
            P(("grp", "sp"), None), P(), P(None, "tp"), P(None, "tp"), P(None, "tp"),
            P("tp", None, None), P("tp", None, None), P("tp"), P("tp", ("grp", "sp")), P("tp"), P("sp", None),
        ),
        out_specs=P(("grp", "sp", "tp"), None),
        check_vma=False,
    )
```

```python
import functools

import jax
import jax.numpy as jnp
from jax import lax
from jax.experimental import pallas as pl
from jax.experimental.pallas import tpu as pltpu
from jax.sharding import PartitionSpec as P

F32 = jnp.float32
BF16 = jnp.bfloat16
BLOCK = 256
SEG = 8
EXTRA = 16
EPS = 1e-06
STREAMS = 2
EXCHANGE = (2, 1, 3, 0)


def on_chip(x):
    return pltpu.with_memory_space_constraint(x, pltpu.VMEM)


def limit(mebibytes):
    return pltpu.CompilerParams(vmem_limit_bytes=mebibytes << 20)


def inverse_norm(rows):
    wide = rows.astype(F32)
    return lax.rsqrt(jnp.mean(wide * wide, axis=1, keepdims=True) + EPS)


def thirds(x):
    top = x.astype(BF16)
    rest = x - top.astype(F32)
    middle = rest.astype(BF16)
    return [top, middle, (rest - middle.astype(F32)).astype(BF16)]


def as_column(row, width):
    pieces = thirds(row) + [jnp.zeros((13, row.shape[1]), BF16)]
    return lax.dot_general(
        jnp.concatenate(pieces, 0), jnp.ones((16, width), BF16), (((0,), (0,)), ((), ())),
        preferred_element_type=F32,
    )


def softplus(x):
    e = jnp.exp(-jnp.abs(x))
    series = 1.0 / 6.0 - e * (1.0 / 7.0)
    for k in (5, 4, 3, 2):
        series = 1.0 / k - e * series
    small = e * (1.0 - e * series)
    return jnp.maximum(x, 0.0) + jnp.where(e < 0.06, small, jnp.log(1.0 + e))


def minus_expm1(y, exp_y):
    series = 1.0 / 120.0 + y * (1.0 / 720.0)
    series = 1.0 / 24.0 + y * series
    series = 1.0 / 6.0 + y * series
    series = 0.5 + y * series
    series = -y * (1.0 + y * series)
    return jnp.where(y > -0.25, series, 1.0 - exp_y)


def gelu(x):
    inner = 0.7978845608028654 * (x + 0.044715 * (x * x * x))
    return 0.5 * x * (1.0 + jnp.tanh(inner))


def logistic(x):
    return 1.0 / (1.0 + jnp.exp(-x))


def shifted_down(x, by, fill):
    rows = lax.broadcasted_iota(jnp.int32, x.shape, 0)
    return jnp.where(rows < by, fill, pltpu.roll(x, by, 0))


def branch_product(rows, weights):
    product = jnp.dot(rows, weights, preferred_element_type=F32)
    return (product * inverse_norm(rows)).astype(BF16)


def scaled_weights(weights, gain):
    return (weights[...].astype(F32) * as_column(gain[...], weights.shape[1])).astype(BF16)


def chunk_copy(source, target, sems, k):
    chunk = source.shape[0] // sems.shape[0]
    at = pl.ds(pl.multiple_of(k * chunk, chunk), chunk)
    return at, pltpu.make_async_copy(source.at[at, :], target.at[at, :], sems.at[k])


def input_kernel(tokens, gain, w_input, projected, scaled, kept, gain_here, w_here, sems, small_sems):
    count = sems.shape[0]
    small = [
        pltpu.make_async_copy(gain, gain_here, small_sems.at[0]),
        pltpu.make_async_copy(w_input, w_here, small_sems.at[1]),
    ]
    for copy in small:
        copy.start()
    for k in range(count):
        chunk_copy(tokens, kept, sems, k)[1].start()
    for copy in small:
        copy.wait()
    scaled[...] = scaled_weights(w_here, gain_here)

    def part(k, _):
        at, copy = chunk_copy(tokens, kept, sems, k)
        copy.wait()
        projected[at, :] = branch_product(kept[at, :], scaled[...])
        return 0

    lax.fori_loop(0, count, part, 0)


def gate_kernel(tokens, gain, w_gate, gate, scaled, kept, made, sems, out_sems):
    count = sems.shape[0]
    for k in range(count):
        chunk_copy(tokens, kept, sems, k)[1].start()
    scaled[...] = scaled_weights(w_gate, gain)

    def part(k, _):
        at, copy = chunk_copy(tokens, kept, sems, k)
        copy.wait()
        made[at, :] = gelu(branch_product(kept[at, :], scaled[...]).astype(F32))
        chunk_copy(made, gate, out_sems, k)[1].start()
        return 0

    lax.fori_loop(0, count, part, 0)
    for k in range(count):
        chunk_copy(made, gate, out_sems, k)[1].wait()


def recur_kernel(projected, taps, w_rate, w_inlet, decay_param, bias, *refs, first):
    if first:
        halo, scaled, refs = *refs[:2], refs[2:]
    else:
        begun, refs = refs[0], refs[3:]
    state_out, prod_out, ends, conv_buf, decay_buf, drive_buf, carry, state, prod, sems = refs
    if first:
        conv_buf[0:8, :] = branch_product(halo[...], scaled[...]).astype(F32)[8:16]
        head_row = lax.broadcasted_iota(jnp.int32, carry.shape, 0) == 0
        carry[...] = jnp.where(head_row, 1.0, 0.0)
    else:
        middle = projected.shape[0] // 2
        conv_buf[0:8, :] = projected[middle - 16 : middle, :].astype(F32)[8:16]
        carry[...] = begun[0]
    soft = softplus(-decay_param[...])
    blocks = projected.shape[0] // 2 // BLOCK
    segs = BLOCK // SEG

    def leaving(k):
        at = (slice(None), pl.ds(pl.multiple_of(k * BLOCK, BLOCK), BLOCK), slice(None))
        block = k + (0 if first else blocks)
        to = (slice(None), pl.ds(pl.multiple_of(block * BLOCK, BLOCK), BLOCK), slice(None))
        return [
            pltpu.make_async_copy(ref.at[at], out.at[to], sems.at[n, k])
            for n, (ref, out) in enumerate(((state, state_out), (prod, prod_out)))
        ]

    def part(k, _):
        block = k + (0 if first else blocks)
        start = pl.multiple_of(block * BLOCK, BLOCK)
        conv_buf[8 : BLOCK + 8, :] = projected[pl.ds(start, BLOCK), :].astype(F32)
        summed = conv_buf[5 : BLOCK + 5, :] * taps[0:1, :]
        for tap in range(1, 4):
            summed = summed + conv_buf[5 + tap : BLOCK + 5 + tap, :] * taps[tap : tap + 1, :]
        conv_buf[0:8, :] = conv_buf[BLOCK : BLOCK + 8, :]
        convolved = summed.astype(BF16)
        rate = logistic(jnp.dot(convolved, w_rate[0], preferred_element_type=F32))
        inlet = logistic(jnp.dot(convolved, w_inlet[0], preferred_element_type=F32))
        log_decay = -8.0 * rate * soft + as_column(bias[0:1, pl.ds(start, BLOCK)], rate.shape[1])
        decay = jnp.exp(log_decay)
        drive = jnp.sqrt(minus_expm1(2.0 * log_decay, decay * decay)) * inlet * convolved.astype(F32)
        for half in range(2):
            lanes = slice(half * 128, half * 128 + 128)
            decay_buf[half] = decay[:, lanes]
            drive_buf[half] = drive[:, lanes]
            row = [(half, pl.ds(r, segs, stride=SEG), slice(None)) for r in range(SEG)]
            p, h = decay_buf[row[0]], drive_buf[row[0]]
            inner = [(p, h)]
            for r in range(1, SEG):
                a = decay_buf[row[r]]
                h = a * h + drive_buf[row[r]]
                p = a * p
                inner.append((p, h))
            by = 1
            while by < segs:
                h = h + p * shifted_down(h, by, 0.0)
                p = p * shifted_down(p, by, 1.0)
                by *= 2
            carry_p, carry_h = carry[0:1, lanes], carry[1:2, lanes]
            start_h = shifted_down(h, 1, 0.0) + shifted_down(p, 1, 1.0) * carry_h
            start_p = shifted_down(p, 1, 1.0) * carry_p
            carry[1:2, lanes] = h[segs - 1 : segs, :] + p[segs - 1 : segs, :] * carry_h
            carry[0:1, lanes] = p[segs - 1 : segs, :] * carry_p
            for r in range(SEG):
                p, h = inner[r]
                at = (half, pl.ds(pl.multiple_of(k * BLOCK, BLOCK) + r, segs, stride=SEG), slice(None))
                state[at] = h + p * start_h
                prod[at] = p * start_p
        for copy in leaving(k):
            copy.start()
        return 0

    lax.fori_loop(0, blocks, part, 0)
    for k in range(blocks):
        for copy in leaving(k):
            copy.wait()
    ends[...] = jnp.broadcast_to(carry[...][None], ends.shape)


def gated_kernel(state, prod, gate, ends, gain, *refs, order):
    count = len(order)
    parts, (incoming, states, prods, gates, sems) = refs[:count], refs[count:]
    seat = lax.axis_index("tp")
    copies = []
    for k, (dx, dc) in enumerate(order):
        to = neighbour(seat, dx, dc, count // 2)
        far = pl.ds(pl.multiple_of(to * BLOCK, BLOCK), BLOCK)
        at = pl.ds(k * BLOCK, BLOCK)
        copies.append(
            [
                pltpu.make_async_copy(state.at[:, far, :], states.at[:, at, :], sems.at[0, k]),
                pltpu.make_async_copy(prod.at[:, far, :], prods.at[:, at, :], sems.at[1, k]),
                pltpu.make_async_copy(gate.at[far, :], gates.at[at, :], sems.at[2, k]),
            ]
        )
        for copy in copies[-1]:
            copy.start()
    span = lax.axis_index("sp")
    total = jnp.zeros((1, gain.shape[1]), F32)
    for k in range(ends.shape[0]):
        total = jnp.where(k < span, ends[k, 0:1, :] * total + ends[k, 1:2, :], total)
    incoming[...] = jnp.broadcast_to(total, incoming.shape)

    ones = jnp.ones((8, 128), BF16)
    over = (((1,), (1,)), ((), ()))
    for k, part in enumerate(parts):
        for copy in copies[k]:
            copy.wait()
        rows = slice(k * BLOCK, k * BLOCK + BLOCK)
        total = jnp.zeros((8, BLOCK), F32)
        for half in range(2):
            lanes = slice(half * 128, half * 128 + 128)
            gated = (states[half, rows, :] + prods[half, rows, :] * incoming[0:1, lanes]) * gates[rows, lanes]
            part[half, 0:BLOCK, :] = (gated * gain[:, lanes]).astype(BF16)
            square = gated * gated
            high = square.astype(BF16)
            low = (square - high.astype(F32)).astype(BF16)
            total = total + lax.dot_general(ones, high, over, preferred_element_type=F32)
            total = total + lax.dot_general(ones, low, over, preferred_element_type=F32)
        top = total.astype(BF16).astype(F32)
        row = lax.broadcasted_iota(jnp.int32, total.shape, 0)
        lines = jnp.where(row == 0, top, jnp.where(row == 1, total - top, 0.0))
        lines = jnp.concatenate([lines, jnp.zeros_like(lines)], 0).astype(BF16)
        for half in range(2):
            part[half, BLOCK : BLOCK + EXTRA, :] = lines[:, half * 128 : half * 128 + 128]


def neighbour(seat, dx, dc, chips):
    return lax_rem(seat // 2 + dx, chips) * 2 + lax_rem(seat % 2 + dc, 2)


def lax_rem(a, b):
    return a % b if isinstance(a, int) else lax.rem(a, b)


def places_of(offsets, spans):
    span, core = lax.axis_index("sp"), lax.axis_index("tp") % 2
    return [lax.rem(span + spans + jnp.where(core == 0, k, -k), spans) for k in offsets]


def grouped(refs, sizes):
    refs = list(refs)
    return [[refs.pop(0) for _ in range(size)] for size in sizes]


def product(arrived, places, groups, low, step):
    mixed = jnp.concatenate([arrived[lax.div(place, 2), lax.rem(place, 2), 0:BLOCK, :] for place in places], 1)
    weights = []
    for parts in groups:
        span = parts[0].shape[1]
        weights.append(parts[low // span][:, low % span : low % span + step])
    return jnp.dot(mixed, jnp.concatenate(weights, 0), preferred_element_type=F32)


def early_kernel(*refs, order, here, away, sizes, spans):
    count = len(order)
    out, arrived, held, sems = refs[-4:]
    outside = refs[-4 - len(away) : -4]
    depth = outside[0].shape[0]
    copies = [
        pltpu.make_async_copy(block, held.at[pl.ds(k * depth, depth), :], sems.at[k])
        for k, block in enumerate(outside)
    ]
    for copy in copies:
        copy.start()
    seat = lax.axis_index("tp")
    for (dx, dc), part in zip(order, refs[:count]):
        arrived[neighbour(seat, count // 2 - dx, dc, count // 2)] = part[...]
    groups = grouped(refs[count:], sizes)
    places = places_of(here, spans)
    step = 512
    for low in range(0, out.shape[1], step):
        out[:, low : low + step] = product(arrived, places, groups, low, step)
    for copy in copies:
        copy.wait()
    places = places_of(away, spans)
    for low in range(0, out.shape[1], step):
        out[:, low : low + step] = out[:, low : low + step] + product(arrived, places, [[held]], low, step)


def middle_kernel(arrived, sums, *refs, offsets, sizes, spans):
    groups, out = grouped(refs, sizes), refs[-1]
    places = places_of(offsets, spans)
    step = 512
    for low in range(0, out.shape[1], step):
        out[:, low : low + step] = sums[:, low : low + step] + product(arrived, places, groups, low, step)


def late_kernel(arrived, sums, near, far, out, *, offset, spans, channels):
    places = places_of([offset], spans)
    core = lax.axis_index("tp") % 2
    ones = jnp.ones((arrived.shape[0] * EXTRA, 128), BF16)
    square = []
    for half in range(2):
        lines = [arrived[k, half, BLOCK : BLOCK + EXTRA, :] for k in range(arrived.shape[0])]
        square.append(
            lax.dot_general(
                jnp.concatenate(lines, 0), ones, (((0,), (0,)), ((), ())), preferred_element_type=F32
            )
        )
    scale = lax.rsqrt(jnp.concatenate(square, 0)[:, 0:1] / channels + EPS)
    step = 512
    span = near.shape[1]
    mixed = arrived[lax.div(places[0], 2), lax.rem(places[0], 2), 0:BLOCK, :]
    for low in range(0, out.shape[1], step):
        at = slice(low % span, low % span + step)
        weights = jnp.where(core == low // span, near[:, at].astype(F32), far[:, at].astype(F32)).astype(BF16)
        acc = sums[:, low : low + step] + jnp.dot(mixed, weights, preferred_element_type=F32)
        out[:, low : low + step] = (acc * scale).astype(BF16)


def tie(*values):
    return lax.optimization_barrier(values)


def body(
    tokens, in_gain, w_input, w_gate, conv_taps, w_rate, w_inlet, decay_param, decay_bias, out_gain, w_out
):
    rows, width = tokens.shape
    head = w_input.shape[1]
    spans, heads = lax.axis_size("sp"), lax.axis_size("tp")
    depth, out_width = w_out.shape
    reach = spans // 2

    around = []
    swap = []
    for z in range(spans):
        for t in range(heads):
            ahead = (z + 1) % spans if t % 2 == 0 else (z - 1) % spans
            around.append((z * heads + t, ahead * heads + t))
            swap.append((z * heads + t, z * heads + t + 1 - 2 * (t % 2)))

    moved, swapped = [], []

    def onward(parts):
        made = []
        for part in parts:
            made.append(lax.ppermute(part, ("sp", "tp"), around))
        moved.append(made)

    def across(parts):
        made = []
        for part in parts:
            made.append(lax.ppermute(part, ("sp", "tp"), swap))
        swapped.append(made)

    def advance(value, pieces=1):
        *value, moved[-1][0] = tie(*value, moved[-1][0])
        parts = moved[-1]
        across(parts)
        if len(parts) < pieces:
            cut = out_width // pieces
            parts = [parts[0][:, k * cut : k * cut + cut] for k in range(pieces)]
        if len(moved) == reach - 1:
            parts = [jnp.where(lax.axis_index("tp") % 2 == 0, *parts)]
        onward(parts)
        return value

    fixed = pl.BlockSpec(memory_space=pltpu.VMEM)
    hbm = pl.BlockSpec(memory_space=pltpu.HBM)
    onward([w_out])
    halo = lax.ppermute(tokens[rows - 16 :], "sp", [(i, i + 1) for i in range(spans - 1)])
    gain_row = in_gain.reshape(1, width)

    in_hbm = lambda x: pltpu.with_memory_space_constraint(x, pltpu.HBM)
    projected, scaled = pl.pallas_call(
        input_kernel,
        in_specs=[hbm] * 3,
        out_specs=[fixed] * 2,
        out_shape=[pltpu.VMEM((rows, head), BF16), pltpu.VMEM((width, head), BF16)],
        scratch_shapes=[
            pltpu.VMEM((rows, width), BF16), pltpu.VMEM((1, width), F32), pltpu.VMEM((width, head), BF16),
            pltpu.SemaphoreType.DMA((4,)), pltpu.SemaphoreType.DMA((2,)),
        ],
        compiler_params=limit(16),
        name="input",
    )(in_hbm(tokens), in_hbm(gain_row), in_hbm(w_input))

    half_rows = rows // 2

    def recur(first, *extra):
        many = 1 if first else spans
        half_shape = (2, half_rows, head // 2)
        return pl.pallas_call(
            functools.partial(recur_kernel, first=first),
            in_specs=[fixed] * (8 if first else 7) + [hbm] * (0 if first else 2),
            out_specs=[hbm, hbm, fixed],
            out_shape=[
                pltpu.HBM((2, rows, head // 2), F32), pltpu.HBM((2, rows, head // 2), F32),
                jax.ShapeDtypeStruct((many, 8, head), F32),
            ],
            scratch_shapes=[
                pltpu.VMEM((BLOCK + 8, head), F32), pltpu.VMEM((2, BLOCK, head // 2), F32),
                pltpu.VMEM((2, BLOCK, head // 2), F32), pltpu.VMEM((8, head), F32),
                pltpu.VMEM(half_shape, F32), pltpu.VMEM(half_shape, F32),
                pltpu.SemaphoreType.DMA((2, half_rows // BLOCK)),
            ],
            input_output_aliases={} if first else {7: 0, 8: 1},
            compiler_params=limit(12),
            name="recur",
        )(on_chip(projected), conv_taps, w_rate, w_inlet, decay_param.reshape(1, head), decay_bias, *extra)

    (projected,) = advance([projected])
    state, prod, begun = recur(True, halo, on_chip(scaled))
    state, prod, ends = recur(False, begun, in_hbm(state), in_hbm(prod))
    (ends,) = advance([ends])
    all_ends = lax.all_to_all(ends, "sp", split_axis=0, concat_axis=0, tiled=True)
    late_tokens, _ = tie(tokens, ends)
    (late_tokens,) = advance([late_tokens])
    gate = pl.pallas_call(
        gate_kernel,
        in_specs=[hbm, fixed, fixed],
        out_specs=hbm,
        out_shape=pltpu.HBM((rows, head), F32),
        scratch_shapes=[
            pltpu.VMEM((width, head), BF16), pltpu.VMEM((rows, width), BF16), pltpu.VMEM((rows, head), F32),
            pltpu.SemaphoreType.DMA((4,)), pltpu.SemaphoreType.DMA((4,)),
        ],
        compiler_params=limit(20),
        name="gate",
    )(in_hbm(late_tokens), gain_row, w_gate)
    order = [(dx, dc) for dx in EXCHANGE for dc in range(2)]
    part_shape = (2, BLOCK + EXTRA, head // 2)
    parts = pl.pallas_call(
        functools.partial(gated_kernel, order=order),
        in_specs=[hbm] * 3 + [fixed] * 2,
        out_specs=[fixed] * heads,
        out_shape=[pltpu.VMEM(part_shape, BF16)] * heads,
        scratch_shapes=[
            pltpu.VMEM((8, head), F32), pltpu.VMEM((2, rows, head // 2), F32),
            pltpu.VMEM((2, rows, head // 2), F32), pltpu.VMEM((rows, head), F32),
            pltpu.SemaphoreType.DMA((3, heads)),
        ],
        compiler_params=limit(12),
        name="gated",
    )(*map(in_hbm, (state, prod, gate)), all_ends, out_gain.reshape(1, head))

    parts = advance(parts, STREAMS)
    moves = []
    for k, (dx, dc) in enumerate(order):
        if (dx, dc) == (1, 0):
            parts = parts[:k] + advance(parts[k:])
        if (dx, dc) == (0, 0):
            parts = parts[:k] + advance(parts[k:])
            moves.append(parts[k])
            continue
        to = lambda t: neighbour(t, dx, dc, heads // 2)
        moves.append(lax.ppermute(parts[k], "tp", [(t, to(t)) for t in range(heads)]))
    (moves[-2],) = advance([moves[-2]])
    across(moved[-1])

    flat = lambda groups: [on_chip(part) for parts in groups for part in parts]
    sizes_of = lambda groups: [len(parts) for parts in groups]
    groups = moved[3:6] + swapped[3:5]
    here = [-4, -5, -6, 4, 5]
    outside = [w_out] + [parts[0] for parts in moved[:3] + swapped[:3]]
    away = [0, -1, -2, -3, 1, 2, 3]
    sums, arrived = pl.pallas_call(
        functools.partial(
            early_kernel, order=order, here=here, away=away, sizes=sizes_of(groups), spans=spans
        ),
        in_specs=[fixed] * (len(moves) + len(flat(groups))) + [hbm] * len(outside),
        out_specs=[fixed] * 2,
        out_shape=[pltpu.VMEM((BLOCK, out_width), F32), pltpu.VMEM((heads, *part_shape), BF16)],
        scratch_shapes=[
            pltpu.VMEM((len(away) * depth, out_width), BF16), pltpu.SemaphoreType.DMA((len(away),)),
        ],
        compiler_params=limit(20),
        name="early",
    )(*map(on_chip, moves), *flat(groups), *map(in_hbm, outside))
    groups = moved[6:7] + swapped[5:7]
    sums = pl.pallas_call(
        functools.partial(middle_kernel, offsets=[-7, 6, 7], sizes=sizes_of(groups), spans=spans),
        in_specs=[fixed] * (2 + len(flat(groups))),
        out_specs=fixed,
        out_shape=pltpu.VMEM((BLOCK, out_width), F32),
        compiler_params=limit(12),
        name="middle",
    )(on_chip(arrived), on_chip(sums), *flat(groups))
    return pl.pallas_call(
        functools.partial(late_kernel, offset=reach, spans=spans, channels=heads * head),
        in_specs=[fixed] * 4,
        out_specs=fixed,
        out_shape=jax.ShapeDtypeStruct((BLOCK, out_width), BF16),
        compiler_params=limit(12),
        name="late",
    )(on_chip(arrived), on_chip(sums), *flat(moved[7:] + swapped[7:]))


def solution(mesh):
    return jax.shard_map(
        body,
        mesh=mesh,
        in_specs=(
            P(("grp", "sp"), None), P(), P(None, "tp"), P(None, "tp"), P(None, "tp"),
            P("tp", None, None), P("tp", None, None), P("tp"), P("tp", ("grp", "sp")), P("tp"), P("sp", None),
        ),
        out_specs=P(("grp", "sp", "tp"), None),
        check_vma=False,
    )
```

```python
import functools

import jax
import jax.numpy as jnp
from jax import lax
from jax.experimental import pallas as pl
from jax.experimental.pallas import tpu as pltpu
from jax.sharding import PartitionSpec as P

F32 = jnp.float32
BF16 = jnp.bfloat16
BLOCK = 256
SEG = 8
EXTRA = 16
EPS = 1e-06
STREAMS = 2
EXCHANGE = (2, 1, 3)


def on_chip(x):
    return pltpu.with_memory_space_constraint(x, pltpu.VMEM)


def limit(mebibytes):
    return pltpu.CompilerParams(vmem_limit_bytes=mebibytes << 20)


def inverse_norm(rows):
    wide = rows.astype(F32)
    return lax.rsqrt(jnp.mean(wide * wide, axis=1, keepdims=True) + EPS)


def thirds(x):
    top = x.astype(BF16)
    rest = x - top.astype(F32)
    middle = rest.astype(BF16)
    return [top, middle, (rest - middle.astype(F32)).astype(BF16)]


def as_column(row, width):
    pieces = thirds(row) + [jnp.zeros((13, row.shape[1]), BF16)]
    return lax.dot_general(
        jnp.concatenate(pieces, 0), jnp.ones((16, width), BF16), (((0,), (0,)), ((), ())),
        preferred_element_type=F32,
    )


def softplus(x):
    e = jnp.exp(-jnp.abs(x))
    series = 1.0 / 6.0 - e * (1.0 / 7.0)
    for k in (5, 4, 3, 2):
        series = 1.0 / k - e * series
    small = e * (1.0 - e * series)
    return jnp.maximum(x, 0.0) + jnp.where(e < 0.06, small, jnp.log(1.0 + e))


def minus_expm1(y, exp_y):
    series = 1.0 / 120.0 + y * (1.0 / 720.0)
    series = 1.0 / 24.0 + y * series
    series = 1.0 / 6.0 + y * series
    series = 0.5 + y * series
    series = -y * (1.0 + y * series)
    return jnp.where(y > -0.25, series, 1.0 - exp_y)


def gelu(x):
    inner = 0.7978845608028654 * (x + 0.044715 * (x * x * x))
    return 0.5 * x * (1.0 + jnp.tanh(inner))


def logistic(x):
    return 1.0 / (1.0 + jnp.exp(-x))


def shifted_down(x, by, fill):
    rows = lax.broadcasted_iota(jnp.int32, x.shape, 0)
    return jnp.where(rows < by, fill, pltpu.roll(x, by, 0))


def branch_product(rows, weights):
    product = jnp.dot(rows, weights, preferred_element_type=F32)
    return (product * inverse_norm(rows)).astype(BF16)


def scaled_weights(weights, gain):
    return (weights[...].astype(F32) * as_column(gain[...], weights.shape[1])).astype(BF16)


def chunk_copy(source, target, sems, k):
    chunk = source.shape[0] // sems.shape[0]
    at = pl.ds(pl.multiple_of(k * chunk, chunk), chunk)
    return at, pltpu.make_async_copy(source.at[at, :], target.at[at, :], sems.at[k])


def input_kernel(tokens, gain, w_input, projected, scaled, kept, gain_here, w_here, sems, small_sems):
    count = sems.shape[0]
    small = [
        pltpu.make_async_copy(gain, gain_here, small_sems.at[0]),
        pltpu.make_async_copy(w_input, w_here, small_sems.at[1]),
    ]
    for copy in small:
        copy.start()
    for k in range(count):
        chunk_copy(tokens, kept, sems, k)[1].start()
    for copy in small:
        copy.wait()
    scaled[...] = scaled_weights(w_here, gain_here)

    def part(k, _):
        at, copy = chunk_copy(tokens, kept, sems, k)
        copy.wait()
        projected[at, :] = branch_product(kept[at, :], scaled[...])
        return 0

    lax.fori_loop(0, count, part, 0)


def gate_kernel(tokens, gain, w_gate, gate, scaled, kept, made, sems, out_sems):
    count = sems.shape[0]
    for k in range(count):
        chunk_copy(tokens, kept, sems, k)[1].start()
    scaled[...] = scaled_weights(w_gate, gain)

    def part(k, _):
        at, copy = chunk_copy(tokens, kept, sems, k)
        copy.wait()
        made[at, :] = gelu(branch_product(kept[at, :], scaled[...]).astype(F32))
        chunk_copy(made, gate, out_sems, k)[1].start()
        return 0

    lax.fori_loop(0, count, part, 0)
    for k in range(count):
        chunk_copy(made, gate, out_sems, k)[1].wait()


def recur_kernel(projected, taps, w_rate, w_inlet, decay_param, bias, *refs, first):
    if first:
        halo, scaled, refs = *refs[:2], refs[2:]
    else:
        begun, refs = refs[0], refs[3:]
    state_out, prod_out, ends, conv_buf, decay_buf, drive_buf, carry, state, prod, sems = refs
    if first:
        conv_buf[0:8, :] = branch_product(halo[...], scaled[...]).astype(F32)[8:16]
        head_row = lax.broadcasted_iota(jnp.int32, carry.shape, 0) == 0
        carry[...] = jnp.where(head_row, 1.0, 0.0)
    else:
        middle = projected.shape[0] // 2
        conv_buf[0:8, :] = projected[middle - 16 : middle, :].astype(F32)[8:16]
        carry[...] = begun[0]
    soft = softplus(-decay_param[...])
    blocks = projected.shape[0] // 2 // BLOCK
    segs = BLOCK // SEG

    def leaving(k):
        at = (slice(None), pl.ds(pl.multiple_of(k * BLOCK, BLOCK), BLOCK), slice(None))
        block = k + (0 if first else blocks)
        to = (slice(None), pl.ds(pl.multiple_of(block * BLOCK, BLOCK), BLOCK), slice(None))
        return [
            pltpu.make_async_copy(ref.at[at], out.at[to], sems.at[n, k])
            for n, (ref, out) in enumerate(((state, state_out), (prod, prod_out)))
        ]

    def part(k, _):
        block = k + (0 if first else blocks)
        start = pl.multiple_of(block * BLOCK, BLOCK)
        conv_buf[8 : BLOCK + 8, :] = projected[pl.ds(start, BLOCK), :].astype(F32)
        summed = conv_buf[5 : BLOCK + 5, :] * taps[0:1, :]
        for tap in range(1, 4):
            summed = summed + conv_buf[5 + tap : BLOCK + 5 + tap, :] * taps[tap : tap + 1, :]
        conv_buf[0:8, :] = conv_buf[BLOCK : BLOCK + 8, :]
        convolved = summed.astype(BF16)
        rate = logistic(jnp.dot(convolved, w_rate[0], preferred_element_type=F32))
        inlet = logistic(jnp.dot(convolved, w_inlet[0], preferred_element_type=F32))
        log_decay = -8.0 * rate * soft + as_column(bias[0:1, pl.ds(start, BLOCK)], rate.shape[1])
        decay = jnp.exp(log_decay)
        drive = jnp.sqrt(minus_expm1(2.0 * log_decay, decay * decay)) * inlet * convolved.astype(F32)
        for half in range(2):
            lanes = slice(half * 128, half * 128 + 128)
            decay_buf[half] = decay[:, lanes]
            drive_buf[half] = drive[:, lanes]
            row = [(half, pl.ds(r, segs, stride=SEG), slice(None)) for r in range(SEG)]
            p, h = decay_buf[row[0]], drive_buf[row[0]]
            inner = [(p, h)]
            for r in range(1, SEG):
                a = decay_buf[row[r]]
                h = a * h + drive_buf[row[r]]
                p = a * p
                inner.append((p, h))
            by = 1
            while by < segs:
                h = h + p * shifted_down(h, by, 0.0)
                p = p * shifted_down(p, by, 1.0)
                by *= 2
            carry_p, carry_h = carry[0:1, lanes], carry[1:2, lanes]
            start_h = shifted_down(h, 1, 0.0) + shifted_down(p, 1, 1.0) * carry_h
            start_p = shifted_down(p, 1, 1.0) * carry_p
            carry[1:2, lanes] = h[segs - 1 : segs, :] + p[segs - 1 : segs, :] * carry_h
            carry[0:1, lanes] = p[segs - 1 : segs, :] * carry_p
            for r in range(SEG):
                p, h = inner[r]
                at = (half, pl.ds(pl.multiple_of(k * BLOCK, BLOCK) + r, segs, stride=SEG), slice(None))
                state[at] = h + p * start_h
                prod[at] = p * start_p
        for copy in leaving(k):
            copy.start()
        return 0

    lax.fori_loop(0, blocks, part, 0)
    for k in range(blocks):
        for copy in leaving(k):
            copy.wait()
    ends[...] = jnp.broadcast_to(carry[0 : ends.shape[1], :][None], ends.shape)


def gated_kernel(state, prod, gate, ends, gain, *refs, order):
    count = len(order)
    kept, given, incoming, states, prods, gates, sems = refs
    seat = lax.axis_index("tp")
    copies = []
    for k, (dx, dc) in enumerate(order):
        to = neighbour(seat, dx, dc, count // 2)
        far = pl.ds(pl.multiple_of(to * BLOCK, BLOCK), BLOCK)
        at = pl.ds(k * BLOCK, BLOCK)
        copies.append(
            [
                pltpu.make_async_copy(state.at[:, far, :], states.at[:, at, :], sems.at[0, k]),
                pltpu.make_async_copy(prod.at[:, far, :], prods.at[:, at, :], sems.at[1, k]),
                pltpu.make_async_copy(gate.at[far, :], gates.at[at, :], sems.at[2, k]),
            ]
        )
        for copy in copies[-1]:
            copy.start()
    span = lax.axis_index("sp")
    total = jnp.zeros((1, gain.shape[1]), F32)
    for k in range(ends.shape[0]):
        total = jnp.where(k < span, ends[k, 0:1, :] * total + ends[k, 1:2, :], total)
    incoming[...] = jnp.broadcast_to(total, incoming.shape)

    ones = jnp.ones((8, 128), BF16)
    over = (((1,), (1,)), ((), ()))
    for k, (dx, dc) in enumerate(order):
        part = (kept, given)[dc].at[dx]
        for copy in copies[k]:
            copy.wait()
        rows = slice(k * BLOCK, k * BLOCK + BLOCK)
        total = jnp.zeros((8, BLOCK), F32)
        for half in range(2):
            lanes = slice(half * 128, half * 128 + 128)
            gated = (states[half, rows, :] + prods[half, rows, :] * incoming[0:1, lanes]) * gates[rows, lanes]
            part[half, 0:BLOCK, :] = (gated * gain[:, lanes]).astype(BF16)
            square = gated * gated
            high = square.astype(BF16)
            low = (square - high.astype(F32)).astype(BF16)
            total = total + lax.dot_general(ones, high, over, preferred_element_type=F32)
            total = total + lax.dot_general(ones, low, over, preferred_element_type=F32)
        top = total.astype(BF16).astype(F32)
        row = lax.broadcasted_iota(jnp.int32, total.shape, 0)
        lines = jnp.where(row == 0, top, jnp.where(row == 1, total - top, 0.0))
        lines = jnp.concatenate([lines, jnp.zeros_like(lines)], 0).astype(BF16)
        for half in range(2):
            part[half, BLOCK : BLOCK + EXTRA, :] = lines[:, half * 128 : half * 128 + 128]


def neighbour(seat, dx, dc, chips):
    return lax_rem(seat // 2 + dx, chips) * 2 + lax_rem(seat % 2 + dc, 2)


def lax_rem(a, b):
    return a % b if isinstance(a, int) else lax.rem(a, b)


def places_of(offsets, spans):
    span, core = lax.axis_index("sp"), lax.axis_index("tp") % 2
    return [lax.rem(span + spans + jnp.where(core == 0, k, -k), spans) for k in offsets]


def grouped(refs, sizes):
    refs = list(refs)
    return [[refs.pop(0) for _ in range(size)] for size in sizes]


def product(arrived, places, groups, low, step):
    mixed = jnp.concatenate([arrived[lax.div(place, 2), lax.rem(place, 2), 0:BLOCK, :] for place in places], 1)
    weights = []
    for parts in groups:
        span = parts[0].shape[1]
        weights.append(parts[low // span][:, low % span : low % span + step])
    return jnp.dot(mixed, jnp.concatenate(weights, 0), preferred_element_type=F32)


def early_kernel(kept, given, *refs, dist, here, away, sizes, away_sizes, spans):
    out, arrived, held, sems = refs[-4:]
    outside = grouped(refs[-4 - sum(away_sizes) : -4], away_sizes)
    depth = outside[0][0].shape[0]
    copies = []
    for k, parts in enumerate(outside):
        for side, part in enumerate(parts):
            width = part.shape[1]
            into = held.at[pl.ds(k * depth, depth), pl.ds(side * width, width)]
            copies.append(pltpu.make_async_copy(part, into, sems.at[len(copies)]))
    for copy in copies:
        copy.start()
    seat = lax.axis_index("tp")
    chips = arrived.shape[0] // 2
    arrived[seat] = kept[0]
    arrived[neighbour(seat, 0, 1, chips)] = given[0]
    for dx, part in zip(dist, refs):
        for side in range(2):
            arrived[neighbour(seat, chips - dx, side, chips)] = part[side]
    groups = grouped(refs[len(dist) :], sizes)
    places = places_of(here, spans)
    step = 512
    for low in range(0, out.shape[1], step):
        out[:, low : low + step] = product(arrived, places, groups, low, step)
    for copy in copies:
        copy.wait()
    places = places_of(away, spans)
    for low in range(0, out.shape[1], step):
        out[:, low : low + step] = out[:, low : low + step] + product(arrived, places, [[held]], low, step)


def middle_kernel(arrived, sums, *refs, offsets, sizes, spans):
    groups, out = grouped(refs, sizes), refs[-1]
    places = places_of(offsets, spans)
    step = 512
    for low in range(0, out.shape[1], step):
        out[:, low : low + step] = sums[:, low : low + step] + product(arrived, places, groups, low, step)


def late_kernel(arrived, sums, near, far, out, *, offset, spans, channels):
    places = places_of([offset], spans)
    core = lax.axis_index("tp") % 2
    ones = jnp.ones((arrived.shape[0] * EXTRA, 128), BF16)
    square = []
    for half in range(2):
        lines = [arrived[k, half, BLOCK : BLOCK + EXTRA, :] for k in range(arrived.shape[0])]
        square.append(
            lax.dot_general(
                jnp.concatenate(lines, 0), ones, (((0,), (0,)), ((), ())), preferred_element_type=F32
            )
        )
    scale = lax.rsqrt(jnp.concatenate(square, 0)[:, 0:1] / channels + EPS)
    step = 512
    span = near.shape[1]
    mixed = arrived[lax.div(places[0], 2), lax.rem(places[0], 2), 0:BLOCK, :]
    for low in range(0, out.shape[1], step):
        at = slice(low % span, low % span + step)
        weights = jnp.where(core == low // span, near[:, at].astype(F32), far[:, at].astype(F32)).astype(BF16)
        acc = sums[:, low : low + step] + jnp.dot(mixed, weights, preferred_element_type=F32)
        out[:, low : low + step] = (acc * scale).astype(BF16)


def tie(*values):
    return lax.optimization_barrier(values)


def body(
    tokens, in_gain, w_input, w_gate, conv_taps, w_rate, w_inlet, decay_param, decay_bias, out_gain, w_out
):
    rows, width = tokens.shape
    head = w_input.shape[1]
    spans, heads = lax.axis_size("sp"), lax.axis_size("tp")
    depth, out_width = w_out.shape
    reach = spans // 2

    around = []
    swap = []
    for z in range(spans):
        for t in range(heads):
            ahead = (z + 1) % spans if t % 2 == 0 else (z - 1) % spans
            around.append((z * heads + t, ahead * heads + t))
            swap.append((z * heads + t, z * heads + t + 1 - 2 * (t % 2)))

    moved, swapped = [], []

    def onward(parts):
        made = []
        for part in parts:
            made.append(lax.ppermute(part, ("sp", "tp"), around))
        moved.append(made)

    def across(parts):
        made = []
        for part in parts:
            made.append(lax.ppermute(part, ("sp", "tp"), swap))
        swapped.append(made)

    def advance(value, pieces=1):
        *value, moved[-1][0] = tie(*value, moved[-1][0])
        parts = moved[-1]
        across(parts)
        if len(parts) < pieces:
            cut = out_width // pieces
            parts = [parts[0][:, k * cut : k * cut + cut] for k in range(pieces)]
        if len(moved) == reach - 1:
            parts = [jnp.where(lax.axis_index("tp") % 2 == 0, *parts)]
        onward(parts)
        return value

    fixed = pl.BlockSpec(memory_space=pltpu.VMEM)
    hbm = pl.BlockSpec(memory_space=pltpu.HBM)
    onward([w_out])
    halo = lax.ppermute(tokens[rows - 16 :], "sp", [(i, i + 1) for i in range(spans - 1)])
    gain_row = in_gain.reshape(1, width)

    in_hbm = lambda x: pltpu.with_memory_space_constraint(x, pltpu.HBM)
    projected, scaled = pl.pallas_call(
        input_kernel,
        in_specs=[hbm] * 3,
        out_specs=[fixed] * 2,
        out_shape=[pltpu.VMEM((rows, head), BF16), pltpu.VMEM((width, head), BF16)],
        scratch_shapes=[
            pltpu.VMEM((rows, width), BF16), pltpu.VMEM((1, width), F32), pltpu.VMEM((width, head), BF16),
            pltpu.SemaphoreType.DMA((4,)), pltpu.SemaphoreType.DMA((2,)),
        ],
        compiler_params=limit(16),
        name="input",
    )(in_hbm(tokens), in_hbm(gain_row), in_hbm(w_input))

    half_rows = rows // 2

    def recur(first, *extra):
        many = (1, 8, head) if first else (spans, 2, head)
        half_shape = (2, half_rows, head // 2)
        return pl.pallas_call(
            functools.partial(recur_kernel, first=first),
            in_specs=[fixed] * (8 if first else 7) + [hbm] * (0 if first else 2),
            out_specs=[hbm, hbm, fixed],
            out_shape=[
                pltpu.HBM((2, rows, head // 2), F32), pltpu.HBM((2, rows, head // 2), F32),
                jax.ShapeDtypeStruct(many, F32),
            ],
            scratch_shapes=[
                pltpu.VMEM((BLOCK + 8, head), F32), pltpu.VMEM((2, BLOCK, head // 2), F32),
                pltpu.VMEM((2, BLOCK, head // 2), F32), pltpu.VMEM((8, head), F32),
                pltpu.VMEM(half_shape, F32), pltpu.VMEM(half_shape, F32),
                pltpu.SemaphoreType.DMA((2, half_rows // BLOCK)),
            ],
            input_output_aliases={} if first else {7: 0, 8: 1},
            compiler_params=limit(12),
            name="recur",
        )(on_chip(projected), conv_taps, w_rate, w_inlet, decay_param.reshape(1, head), decay_bias, *extra)

    (projected,) = advance([projected])
    state, prod, begun = recur(True, halo, on_chip(scaled))
    state, prod, ends = recur(False, begun, in_hbm(state), in_hbm(prod))
    (ends,) = advance([ends])
    all_ends = lax.all_to_all(ends, "sp", split_axis=0, concat_axis=0, tiled=True)
    late_tokens, _ = tie(tokens, ends)
    (late_tokens,) = advance([late_tokens])
    gate = pl.pallas_call(
        gate_kernel,
        in_specs=[hbm, fixed, fixed],
        out_specs=hbm,
        out_shape=pltpu.HBM((rows, head), F32),
        scratch_shapes=[
            pltpu.VMEM((width, head), BF16), pltpu.VMEM((rows, width), BF16), pltpu.VMEM((rows, head), F32),
            pltpu.SemaphoreType.DMA((4,)), pltpu.SemaphoreType.DMA((4,)),
        ],
        compiler_params=limit(20),
        name="gate",
    )(in_hbm(late_tokens), gain_row, w_gate)
    (gate,) = advance([gate], STREAMS)
    chips = heads // 2
    order = [(dx, dc) for dc in (1, 0) for dx in range(chips)]
    part_shape = (2, BLOCK + EXTRA, head // 2)
    kept, given = pl.pallas_call(
        functools.partial(gated_kernel, order=order),
        in_specs=[hbm] * 3 + [fixed] * 2,
        out_specs=[fixed] * 2,
        out_shape=[pltpu.VMEM((chips, *part_shape), BF16)] * 2,
        scratch_shapes=[
            pltpu.VMEM((8, head), F32), pltpu.VMEM((2, rows, head // 2), F32),
            pltpu.VMEM((2, rows, head // 2), F32), pltpu.VMEM((rows, head), F32),
            pltpu.SemaphoreType.DMA((3, heads)),
        ],
        compiler_params=limit(12),
        name="gated",
    )(*map(in_hbm, (state, prod, gate)), all_ends, out_gain.reshape(1, head))

    given = lax.ppermute(given, "tp", [(t, neighbour(t, 0, 1, chips)) for t in range(heads)])
    (kept,) = advance([kept])
    moves = []
    for dx in EXCHANGE:
        both = jnp.stack([kept[dx], given[dx]])
        moves.append(lax.ppermute(both, "tp", [(t, neighbour(t, dx, 0, chips)) for t in range(heads)]))
    while len(moved) < reach:
        (kept,) = advance([kept])
    across(moved[-1])

    flat = lambda groups: [on_chip(part) for parts in groups for part in parts]
    sizes_of = lambda groups: [len(parts) for parts in groups]
    groups = moved[5:6] + swapped[3:5]
    here = [-6, 4, 5]
    outside = [[w_out]] + moved[:5] + swapped[:3]
    away = [0, -1, -2, -3, -4, -5, 1, 2, 3]
    away_sizes = sizes_of(outside)
    sums, arrived = pl.pallas_call(
        functools.partial(
            early_kernel, dist=EXCHANGE, here=here, away=away, sizes=sizes_of(groups),
            away_sizes=away_sizes, spans=spans,
        ),
        in_specs=[fixed] * (2 + len(moves) + len(flat(groups))) + [hbm] * sum(away_sizes),
        out_specs=[fixed] * 2,
        out_shape=[pltpu.VMEM((BLOCK, out_width), F32), pltpu.VMEM((heads, *part_shape), BF16)],
        scratch_shapes=[pltpu.VMEM((len(away) * depth, out_width), BF16), pltpu.SemaphoreType.DMA((sum(away_sizes),))],
        compiler_params=limit(20),
        name="early",
    )(*map(on_chip, (kept, given, *moves)), *flat(groups), *[in_hbm(part) for parts in outside for part in parts])
    groups = moved[6:7] + swapped[5:7]
    sums = pl.pallas_call(
        functools.partial(middle_kernel, offsets=[-7, 6, 7], sizes=sizes_of(groups), spans=spans),
        in_specs=[fixed] * (2 + len(flat(groups))),
        out_specs=fixed,
        out_shape=pltpu.VMEM((BLOCK, out_width), F32),
        compiler_params=limit(12),
        name="middle",
    )(on_chip(arrived), on_chip(sums), *flat(groups))
    return pl.pallas_call(
        functools.partial(late_kernel, offset=reach, spans=spans, channels=heads * head),
        in_specs=[fixed] * 4,
        out_specs=fixed,
        out_shape=jax.ShapeDtypeStruct((BLOCK, out_width), BF16),
        compiler_params=limit(12),
        name="late",
    )(on_chip(arrived), on_chip(sums), *flat(moved[7:] + swapped[7:]))


def solution(mesh):
    return jax.shard_map(
        body,
        mesh=mesh,
        in_specs=(
            P(("grp", "sp"), None), P(), P(None, "tp"), P(None, "tp"), P(None, "tp"),
            P("tp", None, None), P("tp", None, None), P("tp"), P("tp", ("grp", "sp")), P("tp"), P("sp", None),
        ),
        out_specs=P(("grp", "sp", "tp"), None),
        check_vma=False,
    )
```

```python
import functools

import jax
import jax.numpy as jnp
from jax import lax
from jax.experimental import pallas as pl
from jax.experimental.pallas import tpu as pltpu
from jax.sharding import PartitionSpec as P

F32 = jnp.float32
BF16 = jnp.bfloat16
BLOCK = 256
SEG = 8
EXTRA = 16
EPS = 1e-06
STREAMS = 2
EXCHANGE = (2, 1, 3)


def on_chip(x):
    return pltpu.with_memory_space_constraint(x, pltpu.VMEM)


def limit(mebibytes):
    return pltpu.CompilerParams(vmem_limit_bytes=mebibytes << 20)


def inverse_norm(rows):
    wide = rows.astype(F32)
    return lax.rsqrt(jnp.mean(wide * wide, axis=1, keepdims=True) + EPS)


def thirds(x):
    top = x.astype(BF16)
    rest = x - top.astype(F32)
    middle = rest.astype(BF16)
    return [top, middle, (rest - middle.astype(F32)).astype(BF16)]


def as_column(row, width):
    pieces = thirds(row) + [jnp.zeros((13, row.shape[1]), BF16)]
    return lax.dot_general(
        jnp.concatenate(pieces, 0), jnp.ones((16, width), BF16), (((0,), (0,)), ((), ())),
        preferred_element_type=F32,
    )


def softplus(x):
    e = jnp.exp(-jnp.abs(x))
    series = 1.0 / 6.0 - e * (1.0 / 7.0)
    for k in (5, 4, 3, 2):
        series = 1.0 / k - e * series
    small = e * (1.0 - e * series)
    return jnp.maximum(x, 0.0) + jnp.where(e < 0.06, small, jnp.log(1.0 + e))


def minus_expm1(y, exp_y):
    series = 1.0 / 120.0 + y * (1.0 / 720.0)
    series = 1.0 / 24.0 + y * series
    series = 1.0 / 6.0 + y * series
    series = 0.5 + y * series
    series = -y * (1.0 + y * series)
    return jnp.where(y > -0.25, series, 1.0 - exp_y)


def gelu(x):
    inner = 0.7978845608028654 * (x + 0.044715 * (x * x * x))
    return 0.5 * x * (1.0 + jnp.tanh(inner))


def logistic(x):
    return 1.0 / (1.0 + jnp.exp(-x))


def shifted_down(x, by, fill):
    rows = lax.broadcasted_iota(jnp.int32, x.shape, 0)
    return jnp.where(rows < by, fill, pltpu.roll(x, by, 0))


def branch_product(rows, weights):
    product = jnp.dot(rows, weights, preferred_element_type=F32)
    return (product * inverse_norm(rows)).astype(BF16)


def scaled_weights(weights, gain):
    return (weights[...].astype(F32) * as_column(gain[...], weights.shape[1])).astype(BF16)


def chunk_copy(source, target, sems, k):
    chunk = source.shape[0] // sems.shape[0]
    at = pl.ds(pl.multiple_of(k * chunk, chunk), chunk)
    return at, pltpu.make_async_copy(source.at[at, :], target.at[at, :], sems.at[k])


def input_kernel(tokens, gain, w_input, projected, scaled, kept, gain_here, w_here, sems, small_sems):
    count = sems.shape[0]
    small = [
        pltpu.make_async_copy(gain, gain_here, small_sems.at[0]),
        pltpu.make_async_copy(w_input, w_here, small_sems.at[1]),
    ]
    for copy in small:
        copy.start()
    for k in range(count):
        chunk_copy(tokens, kept, sems, k)[1].start()
    for copy in small:
        copy.wait()
    scaled[...] = scaled_weights(w_here, gain_here)

    def part(k, _):
        at, copy = chunk_copy(tokens, kept, sems, k)
        copy.wait()
        projected[at, :] = branch_product(kept[at, :], scaled[...])
        return 0

    lax.fori_loop(0, count, part, 0)


def gate_kernel(tokens, gain, w_gate, gate, scaled, kept, made, sems, out_sems):
    count = sems.shape[0]
    for k in range(count):
        chunk_copy(tokens, kept, sems, k)[1].start()
    scaled[...] = scaled_weights(w_gate, gain)

    def part(k, _):
        at, copy = chunk_copy(tokens, kept, sems, k)
        copy.wait()
        made[at, :] = gelu(branch_product(kept[at, :], scaled[...]).astype(F32))
        chunk_copy(made, gate, out_sems, k)[1].start()
        return 0

    lax.fori_loop(0, count, part, 0)
    for k in range(count):
        chunk_copy(made, gate, out_sems, k)[1].wait()


def recur_kernel(projected, taps, w_rate, w_inlet, decay_param, bias, *refs, first):
    if first:
        halo, scaled, refs = *refs[:2], refs[2:]
    else:
        begun, refs = refs[0], refs[3:]
    state_out, prod_out, ends, conv_buf, decay_buf, drive_buf, carry, state, prod, sems = refs
    if first:
        conv_buf[0:8, :] = branch_product(halo[...], scaled[...]).astype(F32)[8:16]
        head_row = lax.broadcasted_iota(jnp.int32, carry.shape, 0) == 0
        carry[...] = jnp.where(head_row, 1.0, 0.0)
    else:
        middle = projected.shape[0] // 2
        conv_buf[0:8, :] = projected[middle - 16 : middle, :].astype(F32)[8:16]
        carry[...] = begun[0]
    soft = softplus(-decay_param[...])
    blocks = projected.shape[0] // 2 // BLOCK
    segs = BLOCK // SEG

    def leaving(k):
        at = (slice(None), pl.ds(pl.multiple_of(k * BLOCK, BLOCK), BLOCK), slice(None))
        block = k + (0 if first else blocks)
        to = (slice(None), pl.ds(pl.multiple_of(block * BLOCK, BLOCK), BLOCK), slice(None))
        return [
            pltpu.make_async_copy(ref.at[at], out.at[to], sems.at[n, k])
            for n, (ref, out) in enumerate(((state, state_out), (prod, prod_out)))
        ]

    def part(k, _):
        block = k + (0 if first else blocks)
        start = pl.multiple_of(block * BLOCK, BLOCK)
        conv_buf[8 : BLOCK + 8, :] = projected[pl.ds(start, BLOCK), :].astype(F32)
        summed = conv_buf[5 : BLOCK + 5, :] * taps[0:1, :]
        for tap in range(1, 4):
            summed = summed + conv_buf[5 + tap : BLOCK + 5 + tap, :] * taps[tap : tap + 1, :]
        conv_buf[0:8, :] = conv_buf[BLOCK : BLOCK + 8, :]
        convolved = summed.astype(BF16)
        rate = logistic(jnp.dot(convolved, w_rate[0], preferred_element_type=F32))
        inlet = logistic(jnp.dot(convolved, w_inlet[0], preferred_element_type=F32))
        log_decay = -8.0 * rate * soft + as_column(bias[0:1, pl.ds(start, BLOCK)], rate.shape[1])
        decay = jnp.exp(log_decay)
        drive = jnp.sqrt(minus_expm1(2.0 * log_decay, decay * decay)) * inlet * convolved.astype(F32)
        for half in range(2):
            lanes = slice(half * 128, half * 128 + 128)
            decay_buf[half] = decay[:, lanes]
            drive_buf[half] = drive[:, lanes]
            row = [(half, pl.ds(r, segs, stride=SEG), slice(None)) for r in range(SEG)]
            p, h = decay_buf[row[0]], drive_buf[row[0]]
            inner = [(p, h)]
            for r in range(1, SEG):
                a = decay_buf[row[r]]
                h = a * h + drive_buf[row[r]]
                p = a * p
                inner.append((p, h))
            by = 1
            while by < segs:
                h = h + p * shifted_down(h, by, 0.0)
                p = p * shifted_down(p, by, 1.0)
                by *= 2
            carry_p, carry_h = carry[0:1, lanes], carry[1:2, lanes]
            start_h = shifted_down(h, 1, 0.0) + shifted_down(p, 1, 1.0) * carry_h
            start_p = shifted_down(p, 1, 1.0) * carry_p
            carry[1:2, lanes] = h[segs - 1 : segs, :] + p[segs - 1 : segs, :] * carry_h
            carry[0:1, lanes] = p[segs - 1 : segs, :] * carry_p
            for r in range(SEG):
                p, h = inner[r]
                at = (half, pl.ds(pl.multiple_of(k * BLOCK, BLOCK) + r, segs, stride=SEG), slice(None))
                state[at] = h + p * start_h
                prod[at] = p * start_p
        for copy in leaving(k):
            copy.start()
        return 0

    lax.fori_loop(0, blocks, part, 0)
    for k in range(blocks):
        for copy in leaving(k):
            copy.wait()
    ends[...] = jnp.broadcast_to(carry[0 : ends.shape[1], :][None], ends.shape)


def gated_kernel(state, prod, gate, ends, gain, *refs, order):
    count = len(order)
    kept, given, incoming, states, prods, gates, sems = refs
    seat = lax.axis_index("tp")
    copies = []
    for k, (dx, dc) in enumerate(order):
        to = neighbour(seat, dx, dc, count // 2)
        far = pl.ds(pl.multiple_of(to * BLOCK, BLOCK), BLOCK)
        at = pl.ds(k * BLOCK, BLOCK)
        copies.append(
            [
                pltpu.make_async_copy(state.at[:, far, :], states.at[:, at, :], sems.at[0, k]),
                pltpu.make_async_copy(prod.at[:, far, :], prods.at[:, at, :], sems.at[1, k]),
                pltpu.make_async_copy(gate.at[far, :], gates.at[at, :], sems.at[2, k]),
            ]
        )
        for copy in copies[-1]:
            copy.start()
    span = lax.axis_index("sp")
    total = jnp.zeros((1, gain.shape[1]), F32)
    for k in range(ends.shape[0]):
        total = jnp.where(k < span, ends[k, 0:1, :] * total + ends[k, 1:2, :], total)
    incoming[...] = jnp.broadcast_to(total, incoming.shape)

    ones = jnp.ones((8, 128), BF16)
    over = (((1,), (1,)), ((), ()))
    for k, (dx, dc) in enumerate(order):
        part = (kept, given)[dc].at[dx]
        for copy in copies[k]:
            copy.wait()
        rows = slice(k * BLOCK, k * BLOCK + BLOCK)
        total = jnp.zeros((8, BLOCK), F32)
        for half in range(2):
            lanes = slice(half * 128, half * 128 + 128)
            gated = (states[half, rows, :] + prods[half, rows, :] * incoming[0:1, lanes]) * gates[rows, lanes]
            part[half, 0:BLOCK, :] = (gated * gain[:, lanes]).astype(BF16)
            square = gated * gated
            high = square.astype(BF16)
            low = (square - high.astype(F32)).astype(BF16)
            total = total + lax.dot_general(ones, high, over, preferred_element_type=F32)
            total = total + lax.dot_general(ones, low, over, preferred_element_type=F32)
        top = total.astype(BF16).astype(F32)
        row = lax.broadcasted_iota(jnp.int32, total.shape, 0)
        lines = jnp.where(row == 0, top, jnp.where(row == 1, total - top, 0.0))
        lines = jnp.concatenate([lines, jnp.zeros_like(lines)], 0).astype(BF16)
        for half in range(2):
            part[half, BLOCK : BLOCK + EXTRA, :] = lines[:, half * 128 : half * 128 + 128]


def neighbour(seat, dx, dc, chips):
    return lax_rem(seat // 2 + dx, chips) * 2 + lax_rem(seat % 2 + dc, 2)


def lax_rem(a, b):
    return a % b if isinstance(a, int) else lax.rem(a, b)


def places_of(offsets, spans):
    span, core = lax.axis_index("sp"), lax.axis_index("tp") % 2
    return [lax.rem(span + spans + jnp.where(core == 0, k, -k), spans) for k in offsets]


def grouped(refs, sizes):
    refs = list(refs)
    return [[refs.pop(0) for _ in range(size)] for size in sizes]


def product(arrived, places, groups, low, step):
    mixed = jnp.concatenate([arrived[lax.div(place, 2), lax.rem(place, 2), 0:BLOCK, :] for place in places], 1)
    weights = []
    for parts in groups:
        span = parts[0].shape[1]
        weights.append(parts[low // span][:, low % span : low % span + step])
    return jnp.dot(mixed, jnp.concatenate(weights, 0), preferred_element_type=F32)


def pack_kernel(kept, given, *packed, dist):
    for dx, out in zip(dist, packed):
        out[0] = kept[dx]
        out[1] = given[dx]


def early_kernel(kept, given, *refs, dist, here, away, sizes, away_sizes, spans):
    out, arrived, held, sems = refs[-4:]
    outside = grouped(refs[-4 - sum(away_sizes) : -4], away_sizes)
    depth = outside[0][0].shape[0]
    copies = []
    for k, parts in enumerate(outside):
        for side, part in enumerate(parts):
            width = part.shape[1]
            into = held.at[pl.ds(k * depth, depth), pl.ds(side * width, width)]
            copies.append(pltpu.make_async_copy(part, into, sems.at[len(copies)]))
    for copy in copies:
        copy.start()
    seat = lax.axis_index("tp")
    chips = arrived.shape[0] // 2
    arrived[seat] = kept[0]
    arrived[neighbour(seat, 0, 1, chips)] = given[0]
    for dx, part in zip(dist, refs):
        for side in range(2):
            arrived[neighbour(seat, chips - dx, side, chips)] = part[side]
    groups = grouped(refs[len(dist) :], sizes)
    places = places_of(here, spans)
    step = 512
    for low in range(0, out.shape[1], step):
        out[:, low : low + step] = product(arrived, places, groups, low, step)
    for copy in copies:
        copy.wait()
    places = places_of(away, spans)
    for low in range(0, out.shape[1], step):
        out[:, low : low + step] = out[:, low : low + step] + product(arrived, places, [[held]], low, step)


def middle_kernel(arrived, sums, *refs, offsets, sizes, spans):
    groups, out = grouped(refs, sizes), refs[-1]
    places = places_of(offsets, spans)
    step = 512
    for low in range(0, out.shape[1], step):
        out[:, low : low + step] = sums[:, low : low + step] + product(arrived, places, groups, low, step)


def late_kernel(arrived, sums, near, far, out, *, offset, spans, channels):
    places = places_of([offset], spans)
    core = lax.axis_index("tp") % 2
    ones = jnp.ones((arrived.shape[0] * EXTRA, 128), BF16)
    square = []
    for half in range(2):
        lines = [arrived[k, half, BLOCK : BLOCK + EXTRA, :] for k in range(arrived.shape[0])]
        square.append(
            lax.dot_general(
                jnp.concatenate(lines, 0), ones, (((0,), (0,)), ((), ())), preferred_element_type=F32
            )
        )
    scale = lax.rsqrt(jnp.concatenate(square, 0)[:, 0:1] / channels + EPS)
    step = 512
    span = near.shape[1]
    mixed = arrived[lax.div(places[0], 2), lax.rem(places[0], 2), 0:BLOCK, :]
    for low in range(0, out.shape[1], step):
        at = slice(low % span, low % span + step)
        weights = jnp.where(core == low // span, near[:, at].astype(F32), far[:, at].astype(F32)).astype(BF16)
        acc = sums[:, low : low + step] + jnp.dot(mixed, weights, preferred_element_type=F32)
        out[:, low : low + step] = (acc * scale).astype(BF16)


def tie(*values):
    return lax.optimization_barrier(values)


def body(
    tokens, in_gain, w_input, w_gate, conv_taps, w_rate, w_inlet, decay_param, decay_bias, out_gain, w_out
):
    rows, width = tokens.shape
    head = w_input.shape[1]
    spans, heads = lax.axis_size("sp"), lax.axis_size("tp")
    depth, out_width = w_out.shape
    reach = spans // 2

    around = []
    swap = []
    for z in range(spans):
        for t in range(heads):
            ahead = (z + 1) % spans if t % 2 == 0 else (z - 1) % spans
            around.append((z * heads + t, ahead * heads + t))
            swap.append((z * heads + t, z * heads + t + 1 - 2 * (t % 2)))

    moved, swapped = [], []

    def onward(parts):
        made = []
        for part in parts:
            made.append(lax.ppermute(part, ("sp", "tp"), around))
        moved.append(made)

    def across(parts):
        made = []
        for part in parts:
            made.append(lax.ppermute(part, ("sp", "tp"), swap))
        swapped.append(made)

    def advance(value, pieces=1):
        *value, moved[-1][0] = tie(*value, moved[-1][0])
        parts = moved[-1]
        across(parts)
        if len(parts) < pieces:
            cut = out_width // pieces
            parts = [parts[0][:, k * cut : k * cut + cut] for k in range(pieces)]
        if len(moved) == reach - 1:
            parts = [jnp.where(lax.axis_index("tp") % 2 == 0, *parts)]
        onward(parts)
        return value

    fixed = pl.BlockSpec(memory_space=pltpu.VMEM)
    hbm = pl.BlockSpec(memory_space=pltpu.HBM)
    onward([w_out])
    halo = lax.ppermute(tokens[rows - 16 :], "sp", [(i, i + 1) for i in range(spans - 1)])
    gain_row = in_gain.reshape(1, width)

    in_hbm = lambda x: pltpu.with_memory_space_constraint(x, pltpu.HBM)
    projected, scaled = pl.pallas_call(
        input_kernel,
        in_specs=[hbm] * 3,
        out_specs=[fixed] * 2,
        out_shape=[pltpu.VMEM((rows, head), BF16), pltpu.VMEM((width, head), BF16)],
        scratch_shapes=[
            pltpu.VMEM((rows, width), BF16), pltpu.VMEM((1, width), F32), pltpu.VMEM((width, head), BF16),
            pltpu.SemaphoreType.DMA((4,)), pltpu.SemaphoreType.DMA((2,)),
        ],
        compiler_params=limit(16),
        name="input",
    )(in_hbm(tokens), in_hbm(gain_row), in_hbm(w_input))

    half_rows = rows // 2

    def recur(first, *extra):
        many = (1, 8, head) if first else (spans, 2, head)
        half_shape = (2, half_rows, head // 2)
        return pl.pallas_call(
            functools.partial(recur_kernel, first=first),
            in_specs=[fixed] * (8 if first else 7) + [hbm] * (0 if first else 2),
            out_specs=[hbm, hbm, fixed],
            out_shape=[
                pltpu.HBM((2, rows, head // 2), F32), pltpu.HBM((2, rows, head // 2), F32),
                jax.ShapeDtypeStruct(many, F32),
            ],
            scratch_shapes=[
                pltpu.VMEM((BLOCK + 8, head), F32), pltpu.VMEM((2, BLOCK, head // 2), F32),
                pltpu.VMEM((2, BLOCK, head // 2), F32), pltpu.VMEM((8, head), F32),
                pltpu.VMEM(half_shape, F32), pltpu.VMEM(half_shape, F32),
                pltpu.SemaphoreType.DMA((2, half_rows // BLOCK)),
            ],
            input_output_aliases={} if first else {7: 0, 8: 1},
            compiler_params=limit(12),
            name="recur",
        )(on_chip(projected), conv_taps, w_rate, w_inlet, decay_param.reshape(1, head), decay_bias, *extra)

    (projected,) = advance([projected])
    state, prod, begun = recur(True, halo, on_chip(scaled))
    state, prod, ends = recur(False, begun, in_hbm(state), in_hbm(prod))
    (ends,) = advance([ends])
    all_ends = lax.all_to_all(ends, "sp", split_axis=0, concat_axis=0, tiled=True)
    late_tokens, _ = tie(tokens, ends)
    (late_tokens,) = advance([late_tokens])
    gate = pl.pallas_call(
        gate_kernel,
        in_specs=[hbm, fixed, fixed],
        out_specs=hbm,
        out_shape=pltpu.HBM((rows, head), F32),
        scratch_shapes=[
            pltpu.VMEM((width, head), BF16), pltpu.VMEM((rows, width), BF16), pltpu.VMEM((rows, head), F32),
            pltpu.SemaphoreType.DMA((4,)), pltpu.SemaphoreType.DMA((4,)),
        ],
        compiler_params=limit(20),
        name="gate",
    )(in_hbm(late_tokens), gain_row, w_gate)
    (gate,) = advance([gate], STREAMS)
    chips = heads // 2
    order = [(dx, dc) for dc in (1, 0) for dx in range(chips)]
    part_shape = (2, BLOCK + EXTRA, head // 2)
    kept, given = pl.pallas_call(
        functools.partial(gated_kernel, order=order),
        in_specs=[hbm] * 3 + [fixed] * 2,
        out_specs=[fixed] * 2,
        out_shape=[pltpu.VMEM((chips, *part_shape), BF16)] * 2,
        scratch_shapes=[
            pltpu.VMEM((8, head), F32), pltpu.VMEM((2, rows, head // 2), F32),
            pltpu.VMEM((2, rows, head // 2), F32), pltpu.VMEM((rows, head), F32),
            pltpu.SemaphoreType.DMA((3, heads)),
        ],
        compiler_params=limit(12),
        name="gated",
    )(*map(in_hbm, (state, prod, gate)), all_ends, out_gain.reshape(1, head))

    given = lax.ppermute(given, "tp", [(t, neighbour(t, 0, 1, chips)) for t in range(heads)])
    (kept,) = advance([kept])
    packed = pl.pallas_call(
        functools.partial(pack_kernel, dist=EXCHANGE),
        in_specs=[fixed] * 2,
        out_specs=[fixed] * len(EXCHANGE),
        out_shape=[pltpu.VMEM((2, *part_shape), BF16)] * len(EXCHANGE),
        compiler_params=limit(12),
        name="pack",
    )(on_chip(kept), on_chip(given))
    moves = []
    for dx, both in zip(EXCHANGE, packed):
        moves.append(lax.ppermute(both, "tp", [(t, neighbour(t, dx, 0, chips)) for t in range(heads)]))
    while len(moved) < reach:
        (kept,) = advance([kept])
    across(moved[-1])

    flat = lambda groups: [on_chip(part) for parts in groups for part in parts]
    sizes_of = lambda groups: [len(parts) for parts in groups]
    groups = moved[5:6] + swapped[3:5]
    here = [-6, 4, 5]
    outside = [[w_out]] + moved[:5] + swapped[:3]
    away = [0, -1, -2, -3, -4, -5, 1, 2, 3]
    away_sizes = sizes_of(outside)
    sums, arrived = pl.pallas_call(
        functools.partial(
            early_kernel, dist=EXCHANGE, here=here, away=away, sizes=sizes_of(groups),
            away_sizes=away_sizes, spans=spans,
        ),
        in_specs=[fixed] * (2 + len(moves) + len(flat(groups))) + [hbm] * sum(away_sizes),
        out_specs=[fixed] * 2,
        out_shape=[pltpu.VMEM((BLOCK, out_width), F32), pltpu.VMEM((heads, *part_shape), BF16)],
        scratch_shapes=[pltpu.VMEM((len(away) * depth, out_width), BF16), pltpu.SemaphoreType.DMA((sum(away_sizes),))],
        compiler_params=limit(20),
        name="early",
    )(*map(on_chip, (kept, given, *moves)), *flat(groups), *[in_hbm(part) for parts in outside for part in parts])
    groups = moved[6:7] + swapped[5:7]
    sums = pl.pallas_call(
        functools.partial(middle_kernel, offsets=[-7, 6, 7], sizes=sizes_of(groups), spans=spans),
        in_specs=[fixed] * (2 + len(flat(groups))),
        out_specs=fixed,
        out_shape=pltpu.VMEM((BLOCK, out_width), F32),
        compiler_params=limit(12),
        name="middle",
    )(on_chip(arrived), on_chip(sums), *flat(groups))
    return pl.pallas_call(
        functools.partial(late_kernel, offset=reach, spans=spans, channels=heads * head),
        in_specs=[fixed] * 4,
        out_specs=fixed,
        out_shape=jax.ShapeDtypeStruct((BLOCK, out_width), BF16),
        compiler_params=limit(12),
        name="late",
    )(on_chip(arrived), on_chip(sums), *flat(moved[7:] + swapped[7:]))


def solution(mesh):
    return jax.shard_map(
        body,
        mesh=mesh,
        in_specs=(
            P(("grp", "sp"), None), P(), P(None, "tp"), P(None, "tp"), P(None, "tp"),
            P("tp", None, None), P("tp", None, None), P("tp"), P("tp", ("grp", "sp")), P("tp"), P("sp", None),
        ),
        out_specs=P(("grp", "sp", "tp"), None),
        check_vma=False,
    )
```

```python
import functools

import jax
import jax.numpy as jnp
from jax import lax
from jax.experimental import pallas as pl
from jax.experimental.pallas import tpu as pltpu
from jax.sharding import PartitionSpec as P

F32 = jnp.float32
BF16 = jnp.bfloat16
BLOCK = 256
SEG = 8
EXTRA = 16
EPS = 1e-06
STREAMS = 2
EXCHANGE = (2, 1, 3)


def on_chip(x):
    return pltpu.with_memory_space_constraint(x, pltpu.VMEM)


def limit(mebibytes):
    return pltpu.CompilerParams(vmem_limit_bytes=mebibytes << 20)


def inverse_norm(rows):
    wide = rows.astype(F32)
    return lax.rsqrt(jnp.mean(wide * wide, axis=1, keepdims=True) + EPS)


def thirds(x):
    top = x.astype(BF16)
    rest = x - top.astype(F32)
    middle = rest.astype(BF16)
    return [top, middle, (rest - middle.astype(F32)).astype(BF16)]


def as_column(row, width):
    pieces = thirds(row) + [jnp.zeros((13, row.shape[1]), BF16)]
    return lax.dot_general(
        jnp.concatenate(pieces, 0), jnp.ones((16, width), BF16), (((0,), (0,)), ((), ())),
        preferred_element_type=F32,
    )


def softplus(x):
    e = jnp.exp(-jnp.abs(x))
    series = 1.0 / 6.0 - e * (1.0 / 7.0)
    for k in (5, 4, 3, 2):
        series = 1.0 / k - e * series
    small = e * (1.0 - e * series)
    return jnp.maximum(x, 0.0) + jnp.where(e < 0.06, small, jnp.log(1.0 + e))


def minus_expm1(y, exp_y):
    series = 1.0 / 120.0 + y * (1.0 / 720.0)
    series = 1.0 / 24.0 + y * series
    series = 1.0 / 6.0 + y * series
    series = 0.5 + y * series
    series = -y * (1.0 + y * series)
    return jnp.where(y > -0.25, series, 1.0 - exp_y)


def gelu(x):
    inner = 0.7978845608028654 * (x + 0.044715 * (x * x * x))
    return 0.5 * x * (1.0 + jnp.tanh(inner))


def logistic(x):
    return 1.0 / (1.0 + jnp.exp(-x))


def shifted_down(x, by, fill):
    rows = lax.broadcasted_iota(jnp.int32, x.shape, 0)
    return jnp.where(rows < by, fill, pltpu.roll(x, by, 0))


def branch_product(rows, weights):
    product = jnp.dot(rows, weights, preferred_element_type=F32)
    return (product * inverse_norm(rows)).astype(BF16)


def scaled_weights(weights, gain):
    return (weights[...].astype(F32) * as_column(gain[...], weights.shape[1])).astype(BF16)


def chunk_copy(source, target, sems, k):
    chunk = source.shape[0] // sems.shape[0]
    at = pl.ds(pl.multiple_of(k * chunk, chunk), chunk)
    return at, pltpu.make_async_copy(source.at[at, :], target.at[at, :], sems.at[k])


def input_kernel(tokens, gain, w_input, projected, scaled, kept, gain_here, w_here, sems, small_sems):
    count = sems.shape[0]
    small = [
        pltpu.make_async_copy(gain, gain_here, small_sems.at[0]),
        pltpu.make_async_copy(w_input, w_here, small_sems.at[1]),
    ]
    for copy in small:
        copy.start()
    for k in range(2):
        chunk_copy(tokens, kept, sems, k)[1].start()
    for copy in small:
        copy.wait()
    scaled[...] = scaled_weights(w_here, gain_here)

    def part(k, _):
        at, copy = chunk_copy(tokens, kept, sems, k)
        copy.wait()

        @pl.when(k + 2 < count)
        def _():
            chunk_copy(tokens, kept, sems, k + 2)[1].start()

        projected[at, :] = branch_product(kept[at, :], scaled[...])
        return 0

    lax.fori_loop(0, count, part, 0)


def gate_kernel(tokens, gain, w_gate, gate, scaled, kept, made, sems, out_sems):
    count = sems.shape[0]
    for k in range(count):
        chunk_copy(tokens, kept, sems, k)[1].start()
    scaled[...] = scaled_weights(w_gate, gain)

    def part(k, _):
        at, copy = chunk_copy(tokens, kept, sems, k)
        copy.wait()
        made[at, :] = gelu(branch_product(kept[at, :], scaled[...]).astype(F32))
        chunk_copy(made, gate, out_sems, k)[1].start()
        return 0

    lax.fori_loop(0, count, part, 0)
    for k in range(count):
        chunk_copy(made, gate, out_sems, k)[1].wait()


def recur_kernel(projected, taps, w_rate, w_inlet, decay_param, bias, *refs, first):
    if first:
        halo, scaled, refs = *refs[:2], refs[2:]
    else:
        begun, refs = refs[0], refs[3:]
    state_out, prod_out, ends, conv_buf, decay_buf, drive_buf, carry, state, prod, sems = refs
    if first:
        conv_buf[0:8, :] = branch_product(halo[...], scaled[...]).astype(F32)[8:16]
        head_row = lax.broadcasted_iota(jnp.int32, carry.shape, 0) == 0
        carry[...] = jnp.where(head_row, 1.0, 0.0)
    else:
        middle = projected.shape[0] // 2
        conv_buf[0:8, :] = projected[middle - 16 : middle, :].astype(F32)[8:16]
        carry[...] = begun[0]
    soft = softplus(-decay_param[...])
    blocks = projected.shape[0] // 2 // BLOCK
    segs = BLOCK // SEG

    def leaving(k):
        at = (slice(None), pl.ds(pl.multiple_of(k * BLOCK, BLOCK), BLOCK), slice(None))
        block = k + (0 if first else blocks)
        to = (slice(None), pl.ds(pl.multiple_of(block * BLOCK, BLOCK), BLOCK), slice(None))
        return [
            pltpu.make_async_copy(ref.at[at], out.at[to], sems.at[n, k])
            for n, (ref, out) in enumerate(((state, state_out), (prod, prod_out)))
        ]

    def part(k, _):
        block = k + (0 if first else blocks)
        start = pl.multiple_of(block * BLOCK, BLOCK)
        conv_buf[8 : BLOCK + 8, :] = projected[pl.ds(start, BLOCK), :].astype(F32)
        summed = conv_buf[5 : BLOCK + 5, :] * taps[0:1, :]
        for tap in range(1, 4):
            summed = summed + conv_buf[5 + tap : BLOCK + 5 + tap, :] * taps[tap : tap + 1, :]
        conv_buf[0:8, :] = conv_buf[BLOCK : BLOCK + 8, :]
        convolved = summed.astype(BF16)
        rate = logistic(jnp.dot(convolved, w_rate[0], preferred_element_type=F32))
        inlet = logistic(jnp.dot(convolved, w_inlet[0], preferred_element_type=F32))
        log_decay = -8.0 * rate * soft + as_column(bias[0:1, pl.ds(start, BLOCK)], rate.shape[1])
        decay = jnp.exp(log_decay)
        drive = jnp.sqrt(minus_expm1(2.0 * log_decay, decay * decay)) * inlet * convolved.astype(F32)
        for half in range(2):
            lanes = slice(half * 128, half * 128 + 128)
            decay_buf[half] = decay[:, lanes]
            drive_buf[half] = drive[:, lanes]
            row = [(half, pl.ds(r, segs, stride=SEG), slice(None)) for r in range(SEG)]
            p, h = decay_buf[row[0]], drive_buf[row[0]]
            inner = [(p, h)]
            for r in range(1, SEG):
                a = decay_buf[row[r]]
                h = a * h + drive_buf[row[r]]
                p = a * p
                inner.append((p, h))
            by = 1
            while by < segs:
                h = h + p * shifted_down(h, by, 0.0)
                p = p * shifted_down(p, by, 1.0)
                by *= 2
            carry_p, carry_h = carry[0:1, lanes], carry[1:2, lanes]
            start_h = shifted_down(h, 1, 0.0) + shifted_down(p, 1, 1.0) * carry_h
            start_p = shifted_down(p, 1, 1.0) * carry_p
            carry[1:2, lanes] = h[segs - 1 : segs, :] + p[segs - 1 : segs, :] * carry_h
            carry[0:1, lanes] = p[segs - 1 : segs, :] * carry_p
            for r in range(SEG):
                p, h = inner[r]
                at = (half, pl.ds(pl.multiple_of(k * BLOCK, BLOCK) + r, segs, stride=SEG), slice(None))
                state[at] = h + p * start_h
                prod[at] = p * start_p
        for copy in leaving(k):
            copy.start()
        return 0

    lax.fori_loop(0, blocks, part, 0)
    for k in range(blocks):
        for copy in leaving(k):
            copy.wait()
    ends[...] = jnp.broadcast_to(carry[0 : ends.shape[1], :][None], ends.shape)


def gated_kernel(state, prod, gate, ends, gain, *refs, order):
    count = len(order)
    kept, given, incoming, states, prods, gates, sems = refs
    seat = lax.axis_index("tp")
    copies = []
    for k, (dx, dc) in enumerate(order):
        to = neighbour(seat, dx, dc, count // 2)
        far = pl.ds(pl.multiple_of(to * BLOCK, BLOCK), BLOCK)
        at = pl.ds(k * BLOCK, BLOCK)
        copies.append(
            [
                pltpu.make_async_copy(state.at[:, far, :], states.at[:, at, :], sems.at[0, k]),
                pltpu.make_async_copy(prod.at[:, far, :], prods.at[:, at, :], sems.at[1, k]),
                pltpu.make_async_copy(gate.at[far, :], gates.at[at, :], sems.at[2, k]),
            ]
        )
        for copy in copies[-1]:
            copy.start()
    span = lax.axis_index("sp")
    total = jnp.zeros((1, gain.shape[1]), F32)
    for k in range(ends.shape[0]):
        total = jnp.where(k < span, ends[k, 0:1, :] * total + ends[k, 1:2, :], total)
    incoming[...] = jnp.broadcast_to(total, incoming.shape)

    ones = jnp.ones((8, 128), BF16)
    over = (((1,), (1,)), ((), ()))
    for k, (dx, dc) in enumerate(order):
        part = (kept, given)[dc].at[dx]
        for copy in copies[k]:
            copy.wait()
        rows = slice(k * BLOCK, k * BLOCK + BLOCK)
        total = jnp.zeros((8, BLOCK), F32)
        for half in range(2):
            lanes = slice(half * 128, half * 128 + 128)
            gated = (states[half, rows, :] + prods[half, rows, :] * incoming[0:1, lanes]) * gates[rows, lanes]
            part[half, 0:BLOCK, :] = (gated * gain[:, lanes]).astype(BF16)
            square = gated * gated
            high = square.astype(BF16)
            low = (square - high.astype(F32)).astype(BF16)
            total = total + lax.dot_general(ones, high, over, preferred_element_type=F32)
            total = total + lax.dot_general(ones, low, over, preferred_element_type=F32)
        top = total.astype(BF16).astype(F32)
        row = lax.broadcasted_iota(jnp.int32, total.shape, 0)
        lines = jnp.where(row == 0, top, jnp.where(row == 1, total - top, 0.0))
        lines = jnp.concatenate([lines, jnp.zeros_like(lines)], 0).astype(BF16)
        for half in range(2):
            part[half, BLOCK : BLOCK + EXTRA, :] = lines[:, half * 128 : half * 128 + 128]


def neighbour(seat, dx, dc, chips):
    return lax_rem(seat // 2 + dx, chips) * 2 + lax_rem(seat % 2 + dc, 2)


def lax_rem(a, b):
    return a % b if isinstance(a, int) else lax.rem(a, b)


def places_of(offsets, spans):
    span, core = lax.axis_index("sp"), lax.axis_index("tp") % 2
    return [lax.rem(span + spans + jnp.where(core == 0, k, -k), spans) for k in offsets]


def grouped(refs, sizes):
    refs = list(refs)
    return [[refs.pop(0) for _ in range(size)] for size in sizes]


def product(arrived, places, groups, low, step):
    mixed = jnp.concatenate([arrived[lax.div(place, 2), lax.rem(place, 2), 0:BLOCK, :] for place in places], 1)
    weights = []
    for parts in groups:
        span = parts[0].shape[1]
        weights.append(parts[low // span][:, low % span : low % span + step])
    return jnp.dot(mixed, jnp.concatenate(weights, 0), preferred_element_type=F32)


def pack_kernel(kept, given, *packed, dist):
    for dx, out in zip(dist, packed):
        out[0] = kept[dx]
        out[1] = given[dx]


def early_kernel(kept, given, *refs, dist, here, away, sizes, away_sizes, spans):
    out, arrived, held, sems = refs[-4:]
    outside = grouped(refs[-4 - sum(away_sizes) : -4], away_sizes)
    depth = outside[0][0].shape[0]
    copies = []
    for k, parts in enumerate(outside):
        for side, part in enumerate(parts):
            width = part.shape[1]
            into = held.at[pl.ds(k * depth, depth), pl.ds(side * width, width)]
            copies.append(pltpu.make_async_copy(part, into, sems.at[len(copies)]))
    for copy in copies:
        copy.start()
    seat = lax.axis_index("tp")
    chips = arrived.shape[0] // 2
    arrived[seat] = kept[0]
    arrived[neighbour(seat, 0, 1, chips)] = given[0]
    for dx, part in zip(dist, refs):
        for side in range(2):
            arrived[neighbour(seat, chips - dx, side, chips)] = part[side]
    groups = grouped(refs[len(dist) :], sizes)
    places = places_of(here, spans)
    step = 512
    for low in range(0, out.shape[1], step):
        out[:, low : low + step] = product(arrived, places, groups, low, step)
    for copy in copies:
        copy.wait()
    places = places_of(away, spans)
    for low in range(0, out.shape[1], step):
        out[:, low : low + step] = out[:, low : low + step] + product(arrived, places, [[held]], low, step)


def middle_kernel(arrived, sums, *refs, offsets, sizes, spans):
    groups, out = grouped(refs, sizes), refs[-1]
    places = places_of(offsets, spans)
    step = 512
    for low in range(0, out.shape[1], step):
        out[:, low : low + step] = sums[:, low : low + step] + product(arrived, places, groups, low, step)


def late_kernel(arrived, sums, near, far, out, *, offset, spans, channels):
    places = places_of([offset], spans)
    core = lax.axis_index("tp") % 2
    ones = jnp.ones((arrived.shape[0] * EXTRA, 128), BF16)
    square = []
    for half in range(2):
        lines = [arrived[k, half, BLOCK : BLOCK + EXTRA, :] for k in range(arrived.shape[0])]
        square.append(
            lax.dot_general(
                jnp.concatenate(lines, 0), ones, (((0,), (0,)), ((), ())), preferred_element_type=F32
            )
        )
    scale = lax.rsqrt(jnp.concatenate(square, 0)[:, 0:1] / channels + EPS)
    step = 512
    span = near.shape[1]
    mixed = arrived[lax.div(places[0], 2), lax.rem(places[0], 2), 0:BLOCK, :]
    for low in range(0, out.shape[1], step):
        at = slice(low % span, low % span + step)
        weights = jnp.where(core == low // span, near[:, at].astype(F32), far[:, at].astype(F32)).astype(BF16)
        acc = sums[:, low : low + step] + jnp.dot(mixed, weights, preferred_element_type=F32)
        out[:, low : low + step] = (acc * scale).astype(BF16)


def tie(*values):
    return lax.optimization_barrier(values)


def body(
    tokens, in_gain, w_input, w_gate, conv_taps, w_rate, w_inlet, decay_param, decay_bias, out_gain, w_out
):
    rows, width = tokens.shape
    head = w_input.shape[1]
    spans, heads = lax.axis_size("sp"), lax.axis_size("tp")
    depth, out_width = w_out.shape
    reach = spans // 2

    around = []
    swap = []
    for z in range(spans):
        for t in range(heads):
            ahead = (z + 1) % spans if t % 2 == 0 else (z - 1) % spans
            around.append((z * heads + t, ahead * heads + t))
            swap.append((z * heads + t, z * heads + t + 1 - 2 * (t % 2)))

    moved, swapped = [], []

    def onward(parts):
        made = []
        for part in parts:
            made.append(lax.ppermute(part, ("sp", "tp"), around))
        moved.append(made)

    def across(parts):
        made = []
        for part in parts:
            made.append(lax.ppermute(part, ("sp", "tp"), swap))
        swapped.append(made)

    def advance(value, pieces=1):
        *value, moved[-1][0] = tie(*value, moved[-1][0])
        parts = moved[-1]
        across(parts)
        if len(parts) < pieces:
            cut = out_width // pieces
            parts = [parts[0][:, k * cut : k * cut + cut] for k in range(pieces)]
        if len(moved) == reach - 1:
            parts = [jnp.where(lax.axis_index("tp") % 2 == 0, *parts)]
        onward(parts)
        return value

    fixed = pl.BlockSpec(memory_space=pltpu.VMEM)
    hbm = pl.BlockSpec(memory_space=pltpu.HBM)
    onward([w_out])
    halo = lax.ppermute(tokens[rows - 16 :], "sp", [(i, i + 1) for i in range(spans - 1)])
    gain_row = in_gain.reshape(1, width)

    in_hbm = lambda x: pltpu.with_memory_space_constraint(x, pltpu.HBM)
    projected, scaled = pl.pallas_call(
        input_kernel,
        in_specs=[hbm] * 3,
        out_specs=[fixed] * 2,
        out_shape=[pltpu.VMEM((rows, head), BF16), pltpu.VMEM((width, head), BF16)],
        scratch_shapes=[
            pltpu.VMEM((rows, width), BF16), pltpu.VMEM((1, width), F32), pltpu.VMEM((width, head), BF16),
            pltpu.SemaphoreType.DMA((4,)), pltpu.SemaphoreType.DMA((2,)),
        ],
        compiler_params=limit(16),
        name="input",
    )(in_hbm(tokens), in_hbm(gain_row), in_hbm(w_input))

    half_rows = rows // 2

    def recur(first, *extra):
        many = (1, 8, head) if first else (spans, 2, head)
        half_shape = (2, half_rows, head // 2)
        return pl.pallas_call(
            functools.partial(recur_kernel, first=first),
            in_specs=[fixed] * (8 if first else 7) + [hbm] * (0 if first else 2),
            out_specs=[hbm, hbm, fixed],
            out_shape=[
                pltpu.HBM((2, rows, head // 2), F32), pltpu.HBM((2, rows, head // 2), F32),
                jax.ShapeDtypeStruct(many, F32),
            ],
            scratch_shapes=[
                pltpu.VMEM((BLOCK + 8, head), F32), pltpu.VMEM((2, BLOCK, head // 2), F32),
                pltpu.VMEM((2, BLOCK, head // 2), F32), pltpu.VMEM((8, head), F32),
                pltpu.VMEM(half_shape, F32), pltpu.VMEM(half_shape, F32),
                pltpu.SemaphoreType.DMA((2, half_rows // BLOCK)),
            ],
            input_output_aliases={} if first else {7: 0, 8: 1},
            compiler_params=limit(12),
            name="recur",
        )(on_chip(projected), conv_taps, w_rate, w_inlet, decay_param.reshape(1, head), decay_bias, *extra)

    (projected,) = advance([projected])
    state, prod, begun = recur(True, halo, on_chip(scaled))
    state, prod, ends = recur(False, begun, in_hbm(state), in_hbm(prod))
    (ends,) = advance([ends])
    all_ends = lax.all_to_all(ends, "sp", split_axis=0, concat_axis=0, tiled=True)
    late_tokens, _ = tie(tokens, ends)
    (late_tokens,) = advance([late_tokens], STREAMS)
    gate = pl.pallas_call(
        gate_kernel,
        in_specs=[hbm, fixed, fixed],
        out_specs=hbm,
        out_shape=pltpu.HBM((rows, head), F32),
        scratch_shapes=[
            pltpu.VMEM((width, head), BF16), pltpu.VMEM((rows, width), BF16), pltpu.VMEM((rows, head), F32),
            pltpu.SemaphoreType.DMA((4,)), pltpu.SemaphoreType.DMA((4,)),
        ],
        compiler_params=limit(20),
        name="gate",
    )(in_hbm(late_tokens), gain_row, w_gate)
    (gate,) = advance([gate])
    chips = heads // 2
    order = [(dx, dc) for dc in (1, 0) for dx in range(chips)]
    part_shape = (2, BLOCK + EXTRA, head // 2)
    kept, given = pl.pallas_call(
        functools.partial(gated_kernel, order=order),
        in_specs=[hbm] * 3 + [fixed] * 2,
        out_specs=[fixed] * 2,
        out_shape=[pltpu.VMEM((chips, *part_shape), BF16)] * 2,
        scratch_shapes=[
            pltpu.VMEM((8, head), F32), pltpu.VMEM((2, rows, head // 2), F32),
            pltpu.VMEM((2, rows, head // 2), F32), pltpu.VMEM((rows, head), F32),
            pltpu.SemaphoreType.DMA((3, heads)),
        ],
        compiler_params=limit(12),
        name="gated",
    )(*map(in_hbm, (state, prod, gate)), all_ends, out_gain.reshape(1, head))

    given = lax.ppermute(given, "tp", [(t, neighbour(t, 0, 1, chips)) for t in range(heads)])
    (kept,) = advance([kept])
    packed = pl.pallas_call(
        functools.partial(pack_kernel, dist=EXCHANGE),
        in_specs=[fixed] * 2,
        out_specs=[fixed] * len(EXCHANGE),
        out_shape=[pltpu.VMEM((2, *part_shape), BF16)] * len(EXCHANGE),
        compiler_params=limit(12),
        name="pack",
    )(on_chip(kept), on_chip(given))
    moves = []
    for dx, both in zip(EXCHANGE, packed):
        moves.append(lax.ppermute(both, "tp", [(t, neighbour(t, dx, 0, chips)) for t in range(heads)]))
    while len(moved) < reach:
        (kept,) = advance([kept])
    across(moved[-1])

    flat = lambda groups: [on_chip(part) for parts in groups for part in parts]
    sizes_of = lambda groups: [len(parts) for parts in groups]
    groups = moved[5:6] + swapped[3:5]
    here = [-6, 4, 5]
    outside = [[w_out]] + moved[:5] + swapped[:3]
    away = [0, -1, -2, -3, -4, -5, 1, 2, 3]
    away_sizes = sizes_of(outside)
    sums, arrived = pl.pallas_call(
        functools.partial(
            early_kernel, dist=EXCHANGE, here=here, away=away, sizes=sizes_of(groups),
            away_sizes=away_sizes, spans=spans,
        ),
        in_specs=[fixed] * (2 + len(moves) + len(flat(groups))) + [hbm] * sum(away_sizes),
        out_specs=[fixed] * 2,
        out_shape=[pltpu.VMEM((BLOCK, out_width), F32), pltpu.VMEM((heads, *part_shape), BF16)],
        scratch_shapes=[pltpu.VMEM((len(away) * depth, out_width), BF16), pltpu.SemaphoreType.DMA((sum(away_sizes),))],
        compiler_params=limit(20),
        name="early",
    )(*map(on_chip, (kept, given, *moves)), *flat(groups), *[in_hbm(part) for parts in outside for part in parts])
    groups = moved[6:7] + swapped[5:7]
    sums = pl.pallas_call(
        functools.partial(middle_kernel, offsets=[-7, 6, 7], sizes=sizes_of(groups), spans=spans),
        in_specs=[fixed] * (2 + len(flat(groups))),
        out_specs=fixed,
        out_shape=pltpu.VMEM((BLOCK, out_width), F32),
        compiler_params=limit(12),
        name="middle",
    )(on_chip(arrived), on_chip(sums), *flat(groups))
    return pl.pallas_call(
        functools.partial(late_kernel, offset=reach, spans=spans, channels=heads * head),
        in_specs=[fixed] * 4,
        out_specs=fixed,
        out_shape=jax.ShapeDtypeStruct((BLOCK, out_width), BF16),
        compiler_params=limit(12),
        name="late",
    )(on_chip(arrived), on_chip(sums), *flat(moved[7:] + swapped[7:]))


def solution(mesh):
    return jax.shard_map(
        body,
        mesh=mesh,
        in_specs=(
            P(("grp", "sp"), None), P(), P(None, "tp"), P(None, "tp"), P(None, "tp"),
            P("tp", None, None), P("tp", None, None), P("tp"), P("tp", ("grp", "sp")), P("tp"), P("sp", None),
        ),
        out_specs=P(("grp", "sp", "tp"), None),
        check_vma=False,
    )
```
